128 devices in a mesh: ep: 64 (over z, y, x), tp: 2 (over core).
Axes of the slice: x: 4, y: 4, z: 4, core: 2. Of those that a mesh axis runs over, the one named last changes fastest.
Arguments:
- hidden_in: bfloat16 [2048, 2048], P('ep'), may hold values from -6 to 6
- past_lengths: int32 [2048], P('ep'), may hold values from 1 to 1023, as said below
- key_cache: bfloat16 [2048, 1024, 256], P('ep', None, 'tp'), may hold values from -512 to 512
- value_cache: bfloat16 [2048, 1024, 256], P('ep', None, 'tp'), may hold values from -6 to 6
- attn_gain: float32 [2048], replicated, may hold values from 0.1 to 1.9
- w_query: bfloat16 [2048, 2048], P(None, 'tp'), may hold values from -0.125 to 0.125
- w_key: bfloat16 [2048, 256], P(None, 'tp'), may hold values from -0.125 to 0.125
- w_value: bfloat16 [2048, 256], P(None, 'tp'), may hold values from -0.125 to 0.125
- lambdas: float32 [16], P('tp'), may hold values from 0.3 to 0.8
- head_gain: float32 [128], replicated, may hold values from 0.1 to 1.9
- w_out: bfloat16 [2048, 2048], P('tp'), may hold values from -0.125 to 0.125
- ffn_gain: float32 [2048], replicated, may hold values from 0.1 to 1.9
- route_ids: int32 [2048, 2], P('ep'), may hold values from 0 to 31, all different within a row; in each aligned block of 32 rows (0 to 31, 32 to 63, ...) at most 4 rows name the same one
- route_weights: float32 [2048, 2], P('ep'), may hold values from 0.2 to 1
- expert_gate: bfloat16 [64, 2048, 704], P('ep', None, 'tp'), may hold values from -0.125 to 0.125
- expert_up: bfloat16 [64, 2048, 704], P('ep', None, 'tp'), may hold values from -0.125 to 0.125
- expert_down: bfloat16 [64, 704, 2048], P('ep', None, 'tp'), may hold values from -1.25 to 1.25
- gate_vector: bfloat16 [2048], replicated, may hold values from -0.125 to 0.125
- dense_gate: bfloat16 [2048, 5632], P(None, ('ep', 'tp')), may hold values from -0.125 to 0.125
- dense_up: bfloat16 [2048, 5632], P(None, ('ep', 'tp')), may hold values from -0.125 to 0.125
- dense_down: bfloat16 [5632, 2048], P('ep', 'tp'), may hold values from -0.625 to 0.625
Outputs:
- mixed_out: bfloat16 [2048, 2048], P('ep', 'tp')
- new_keys: bfloat16 [2048, 256], P('ep', 'tp')
- new_values: bfloat16 [2048, 256], P('ep', 'tp')
The draws below stay inside these ranges and needn't reach their ends.
Inputs may be any that keep to these rules, and one draw needn't show every extreme that they name: `past_lengths`: the new token of a sequence stands at this position; some sequence has 1023 cached positions in every draw. `route_ids`: each row names 2 different experts; among the rows of one index of ep no expert is named more than 4 times, a bound that some block reaches in every draw.
All inputs are finite; a program needn't handle non-finite values.
Results may differ from the reference program's by a relative error of at most 0.02.
The reference program's roundings to bfloat16 on the way count: a program that leaves them out, or rounds other values in their place, can miss the bound.
Values may be sent and summed in bfloat16 or wider, within the bound.
A program may use at most 128 MiB of HBM per device.

```python
import math
import jax
import jax.numpy as jnp
import numpy as np
from jax import lax

D = 2048
HEADS = 16
KV_HEADS = 2
HEAD_DIM = 64
VALUE_DIM = 128
EXPERT_W = 1408
FF_DENSE = 5632
TOP = 2
CACHE_LEN = 1024
SEQ_GRP = 32
EXPERTS = 32
CAP = 4
SEQS = 2048
N_EP = 64
N_TP = 2


def draw_past_lengths(key, part):
    key_top, key_share, key_pick = jax.random.split(jax.random.fold_in(key, 71), 3)
    groups = SEQS // SEQ_GRP
    reach_top = jax.random.randint(key_top, (groups, 1), CACHE_LEN // 8, CACHE_LEN)
    shares = jax.random.randint(key_share, (groups, SEQ_GRP), 0, 65536)
    lengths = (1 + (reach_top - 1) * shares // 65536).reshape(-1)
    chosen = jax.random.randint(key_pick, (), 0, SEQS)
    return jnp.where(jnp.arange(SEQS) == chosen, CACHE_LEN - 1, lengths).astype(jnp.int32)


def draw_key_cache(key, part):
    key_drawn = jax.random.fold_in(jax.random.fold_in(key, 73), 0)
    extent = (SEQS, CACHE_LEN, KV_HEADS * 2 * HEAD_DIM)
    drawn_keys = jax.random.truncated_normal(key_drawn, -4.0, 4.0, extent, jnp.float32) * 1.7
    return drawn_keys.astype(jnp.bfloat16)


def shard_levels(own_key, dims, cuts, least, high):
    loudness = 1.0
    for dim, blocks in cuts:
        draws = jax.random.uniform(jax.random.fold_in(jax.random.fold_in(own_key, 6), dim), (blocks,), jnp.float32, least / len(cuts), high / len(cuts))
        loudness = loudness * jnp.repeat(jnp.exp(draws), dims[dim] // blocks).reshape((-1,) + (1,) * (len(dims) - 1 - dim))
    return loudness


def routed_block(stream_key, own, number, rows, number_of, top, limit, slope):
    sequence = jax.random.permutation(stream_key, number_of)
    crowded, usual = portions_of(number_of, rows * top, limit, slope, True), portions_of(number_of, rows * top, limit, slope, False)
    places = jnp.arange(number_of)

    def named(sizes, turn):
        used = int((sizes > 0).sum())
        fixed = max(1, used // 4)
        moved = fixed + (places - fixed + turn * (used - fixed)) % max(1, number_of - fixed)
        return jnp.zeros((number_of,), jnp.int32).at[sequence[jnp.where(places < fixed, places, moved)]].set(jnp.asarray(sizes, jnp.int32))

    sizes = jnp.where(number % 4 == 0, named(crowded, number // 4), named(usual, number - number // 4 - 1))
    mixed = jax.random.permutation(jax.random.fold_in(own, 3), number_of)
    giver, sink = mixed[0:number_of // 2 * 2:2], mixed[1:number_of // 2 * 2:2]
    room = jnp.minimum(sizes[giver] - 1, limit - sizes[sink]) // 2
    room = jnp.where((giver == sequence[0]) | (sink == sequence[0]) | (sizes[sink] == 0), 0, jnp.maximum(room, 0))
    moved = jax.random.randint(jax.random.fold_in(own, 4), (number_of // 2,), 0, 1 << 20) % (room + 1)
    sizes = sizes.at[giver].add(-moved).at[sink].add(moved)
    items = jnp.searchsorted(jnp.cumsum(sizes), jnp.arange(rows * top), side="right").astype(jnp.int32)
    grid = items.reshape(top, rows).T
    grid = grid[jax.random.permutation(jax.random.fold_in(own, 1), rows)]
    turn = jax.random.randint(jax.random.fold_in(own, 2), (rows, 1), 0, top)
    return jnp.take_along_axis(grid, (jnp.arange(top)[None, :] + turn) % top, axis=1)


def portions_of(amount, total, limit, slope, full):
    loads = [(1 << 20) // math.isqrt(rank ** slope) + 1 for rank in range(1, amount + 1)]
    largest = limit if full else min(limit, max(-(-total // amount), total * loads[0] // sum(loads)))
    least = 1 if total - largest >= amount - 1 else 0
    given, spare = [largest] + [least] * (amount - 1), total - largest - least * (amount - 1)
    while spare > 0:
        movable = [i for i in range(1, amount) if given[i] < largest] or [i for i in range(1, amount) if given[i] < limit]
        pool, left = sum([loads[i] for i in movable]), spare
        for i in movable:
            addition = min(limit - given[i], max(1, left * loads[i] // pool), spare)
            given[i] = given[i] + addition
            spare = spare - addition
    return np.array(given)


def noise(own_key, shape, spread, bound, pieces=(), held_as=jnp.bfloat16):
    gain = shard_levels(own_key, shape, pieces, -0.22, 0.18) if pieces else 1.0
    values = jax.random.normal(own_key, shape, jnp.float32) * spread * gain
    return jnp.minimum(jnp.maximum(values, -bound), bound).astype(held_as)


def setup_inputs(seed: int = 0) -> dict:
    key_of = jax.random.split(jax.random.key(seed), 22)
    hidden_in = noise(key_of[0], (SEQS, D), 1.0, 6.0, ((0, 64),))
    past_lengths = draw_past_lengths(jax.random.fold_in(key_of[21], 71), 0)
    key_cache = draw_key_cache(jax.random.fold_in(key_of[21], 71), 0)
    value_cache = noise(key_of[3], (SEQS, CACHE_LEN, KV_HEADS * VALUE_DIM), 1.0, 6.0, ((0, 64), (2, 2)))
    attn_gain = jnp.clip(1.0 + 0.18 * jax.random.normal(key_of[4], (D,), jnp.float32), 0.1, 1.9)
    w_query = noise(key_of[5], (D, HEADS * 2 * HEAD_DIM), D ** -0.5, 0.125, ((1, 2),))
    w_key = noise(key_of[6], (D, KV_HEADS * 2 * HEAD_DIM), D ** -0.5, 0.125, ((1, 2),))
    w_value = noise(key_of[7], (D, KV_HEADS * VALUE_DIM), D ** -0.5, 0.125, ((1, 2),))
    lambdas = jnp.clip(0.3 + 0.5 * jax.random.uniform(key_of[8], (HEADS,), jnp.float32) ** shard_levels(key_of[8], (HEADS,), ((0, 2),), -0.2, 0.2), 0.3, 0.8)
    head_gain = jnp.clip(1.0 + 0.18 * jax.random.normal(key_of[9], (VALUE_DIM,), jnp.float32), 0.1, 1.9)
    w_out = noise(key_of[10], (HEADS * VALUE_DIM, D), (HEADS * VALUE_DIM) ** -0.5, 0.125, ((0, 2),))
    ffn_gain = jnp.clip(1.0 + 0.18 * jax.random.normal(key_of[11], (D,), jnp.float32), 0.1, 1.9)
    route_ids_keys = jax.random.split(jax.random.fold_in(key_of[12], 1), SEQS // SEQ_GRP)
    route_ids_turns = jax.random.permutation(jax.random.fold_in(key_of[12], 3), SEQS // SEQ_GRP)
    route_ids = jax.vmap(lambda own, number: routed_block(jax.random.fold_in(key_of[12], 2), own, number, SEQ_GRP, EXPERTS, TOP, CAP, 2))(route_ids_keys, route_ids_turns).reshape((SEQS, TOP))
    route_weights = jnp.clip(0.2 + 0.8 * jax.random.uniform(key_of[13], (SEQS, TOP), jnp.float32) ** shard_levels(key_of[13], (SEQS, TOP), ((0, 64),), -0.2, 0.2), 0.2, 1.0)
    expert_gate = noise(key_of[14], (2 * EXPERTS, D, EXPERT_W // 2), D ** -0.5, 0.125, ((0, 64), (2, 2)))
    expert_up = noise(key_of[15], (2 * EXPERTS, D, EXPERT_W // 2), D ** -0.5, 0.125, ((0, 64), (2, 2)))
    expert_down = noise(key_of[16], (2 * EXPERTS, EXPERT_W // 2, D), (3.0 * EXPERT_W ** -0.5), 1.25, ((0, 64), (2, 2)))
    gate_vector = noise(key_of[17], (D,), D ** -0.5, 0.125)
    dense_gate = noise(key_of[18], (D, FF_DENSE), D ** -0.5, 0.125, ((1, 128),))
    dense_up = noise(key_of[19], (D, FF_DENSE), D ** -0.5, 0.125, ((1, 128),))
    dense_down = noise(key_of[20], (FF_DENSE, D), (3.0 * FF_DENSE ** -0.5), 0.625, ((0, 64), (1, 2)))
    return dict(hidden_in=hidden_in, past_lengths=past_lengths, key_cache=key_cache, value_cache=value_cache, attn_gain=attn_gain, w_query=w_query, w_key=w_key, w_value=w_value, lambdas=lambdas, head_gain=head_gain, w_out=w_out, ffn_gain=ffn_gain, route_ids=route_ids, route_weights=route_weights, expert_gate=expert_gate, expert_up=expert_up, expert_down=expert_down, gate_vector=gate_vector, dense_gate=dense_gate, dense_up=dense_up, dense_down=dense_down)


norm_eps = 1e-05
rope_base = 10000.0

def rms_rows(values, scales):
    values = values.astype(jnp.float32)
    return values * lax.rsqrt(lax.optimization_barrier(jnp.mean(values * values, axis=-1, keepdims=True)) + norm_eps) * scales

def rotary(values, position):
    middle = values.shape[-1] // 2
    inverse = rope_base ** (-jnp.arange(middle, dtype=jnp.float32) / middle)
    angles = position.astype(jnp.float32)[:, None] * inverse[None, :]
    cosine = jnp.cos(angles)[:, None, None, :]
    sine_part = jnp.sin(angles)[:, None, None, :]
    leading, second = (values[..., :middle], values[..., middle:])
    return jnp.concatenate([leading * cosine - second * sine_part, second * cosine + leading * sine_part], axis=-1)

def rounded(values):
    return lax.optimization_barrier(values.astype(jnp.bfloat16)).astype(jnp.float32)

def reference(hidden_in, past_lengths, key_cache, value_cache, attn_gain, w_query, w_key, w_value, lambdas, head_gain, w_out, ffn_gain, route_ids, route_weights, expert_gate, expert_up, expert_down, gate_vector, dense_gate, dense_up, dense_down):
    batch_rows = hidden_in.shape[0]
    normed = rms_rows(hidden_in, attn_gain).astype(jnp.bfloat16)
    queries = rotary(jnp.dot(normed, w_query, preferred_element_type=jnp.float32).reshape(batch_rows, HEADS, 2, HEAD_DIM), past_lengths).astype(jnp.bfloat16)
    key_new = rotary(jnp.dot(normed, w_key, preferred_element_type=jnp.float32).reshape(batch_rows, KV_HEADS, 2, HEAD_DIM), past_lengths).astype(jnp.bfloat16)
    value_new = jnp.dot(normed, w_value, preferred_element_type=jnp.float32).astype(jnp.bfloat16)
    per_key = HEADS // KV_HEADS
    scale_qk = HEAD_DIM ** (-0.5)

    def attend(packed):
        query_seq, key_seq, value_seq, cache_keys, cache_values, length = packed
        grouped = query_seq.reshape(KV_HEADS, per_key, 2, HEAD_DIM).astype(jnp.float32)
        key_rows = cache_keys.reshape(CACHE_LEN, KV_HEADS, 2, HEAD_DIM).astype(jnp.float32)
        value_rows = cache_values.reshape(CACHE_LEN, KV_HEADS, VALUE_DIM).astype(jnp.float32)
        scores = jnp.einsum('gamd,lgmd->gaml', grouped, key_rows) * scale_qk
        own_score = jnp.einsum('gamd,gmd->gam', grouped, key_seq.astype(jnp.float32)) * scale_qk
        usable = jnp.arange(CACHE_LEN) < length
        scores = jnp.where(usable, scores, -jnp.inf)
        highest = jnp.maximum(lax.optimization_barrier(jnp.max(scores, axis=-1)), own_score)
        weights = jnp.exp(scores - highest[..., None])
        own_weight = jnp.exp(own_score - highest)
        totals = lax.optimization_barrier(jnp.sum(weights, axis=-1)) + own_weight
        summed = jnp.einsum('gaml,lge->game', rounded(weights), value_rows)
        summed = summed + rounded(own_weight)[..., None] * value_seq.reshape(KV_HEADS, 1, 1, VALUE_DIM).astype(jnp.float32)
        return (summed / totals[..., None]).reshape(HEADS, 2, VALUE_DIM)
    mapped = lax.map(attend, (queries, key_new, value_new, key_cache, value_cache, past_lengths))
    head_mix = mapped[:, :, 0] - lambdas[None, :, None] * mapped[:, :, 1]
    head_out = rms_rows(head_mix, head_gain).astype(jnp.bfloat16).reshape(batch_rows, N_TP, -1)
    out_rows = w_out.reshape(N_TP, -1, D)
    partials = jnp.einsum('sgk,gkd->sgd', head_out.astype(jnp.float32), out_rows.astype(jnp.float32))
    attn_out = lax.optimization_barrier(jnp.sum(rounded(partials), axis=1)).astype(jnp.bfloat16)
    residual = hidden_in.astype(jnp.float32) + attn_out.astype(jnp.float32)
    moe_in = rms_rows(residual, ffn_gain).astype(jnp.bfloat16)
    mix_gate = jax.nn.sigmoid(jnp.dot(moe_in, gate_vector, preferred_element_type=jnp.float32)).astype(jnp.bfloat16)
    slot_count = N_EP * CAP
    gate_pairs = expert_gate.reshape(EXPERTS, 2, D, -1)
    up_pairs = expert_up.reshape(EXPERTS, 2, D, -1)
    down_pairs = expert_down.reshape(EXPERTS, 2, -1, D)

    def add_expert(expert, moe_total):
        matches = route_ids == expert
        weight = lax.optimization_barrier(jnp.sum(jnp.where(matches, route_weights, 0.0), axis=1))
        chosen = jnp.any(matches, axis=1)
        number = jnp.sum(chosen.astype(jnp.int32))
        picked = jnp.nonzero(chosen, size=slot_count, fill_value=0)[0]
        live_slot = (jnp.arange(slot_count) < number).astype(jnp.float32)
        taken = moe_in[picked]
        gates_here = lax.dynamic_index_in_dim(gate_pairs, expert, 0, keepdims=False)
        ups_here = lax.dynamic_index_in_dim(up_pairs, expert, 0, keepdims=False)
        downs_here = lax.dynamic_index_in_dim(down_pairs, expert, 0, keepdims=False)
        result = jnp.zeros((slot_count, D), jnp.float32)
        for half_index in range(2):
            gate_pre = jnp.dot(taken, gates_here[half_index], preferred_element_type=jnp.float32)
            up_pre = jnp.dot(taken, ups_here[half_index], preferred_element_type=jnp.float32)
            inner_act = (jax.nn.silu(gate_pre) * up_pre).astype(jnp.bfloat16)
            result = result + jnp.dot(inner_act, downs_here[half_index], preferred_element_type=jnp.float32)
        return moe_total.at[picked].add(result * (weight[picked] * live_slot)[:, None])
    moe_out = lax.fori_loop(0, EXPERTS, add_expert, jnp.zeros((batch_rows, D), jnp.float32))
    dense_pre = jnp.dot(moe_in, dense_gate, preferred_element_type=jnp.float32)
    dense_upper = jnp.dot(moe_in, dense_up, preferred_element_type=jnp.float32)
    dense_act = (jax.nn.silu(dense_pre) * dense_upper).astype(jnp.bfloat16)
    dense_out = jnp.dot(dense_act, dense_down, preferred_element_type=jnp.float32) * mix_gate.astype(jnp.float32)[:, None]
    mixed_out = (residual + moe_out + dense_out).astype(jnp.bfloat16)
    return (mixed_out, key_new.reshape(batch_rows, -1), value_new)
```

```python
import functools

import jax
import jax.numpy as jnp
from jax import lax
from jax.experimental import pallas as pl
from jax.experimental.pallas import tpu as pltpu
from jax.sharding import PartitionSpec as P

EPS = 1e-05
ROPE_BASE = 10000.0
BF = jnp.bfloat16
F32 = jnp.float32
ROWS = 32
WIDTH = 2048
HALF = 1024
CACHE = 1024
GRP = 4
NGRP = ROWS // GRP
NT = (((1,), (1,)), ((), ()))
TN = (((0,), (0,)), ((), ()))


def dot(a, b):
    return jnp.dot(a, b, preferred_element_type=F32)


def dot_nt(a, b):
    return lax.dot_general(a, b, NT, preferred_element_type=F32)


def dot_tn(a, b):
    return lax.dot_general(a, b, TN, preferred_element_type=F32)


def layer_kernel(
    hid, trig, plen, again, lam, hgain, fgain, route,
    kc_h, vc_h, wq_h, wk_h, wv_h, wo_h, eg_h, eu_h, ed_h, wd_h, dd_h,
    out, nk, nv,
    kb, vb, wq, wk, wv, wo, eg, eu, ed,
    wdg, ddg, qs, kn, vn, ho, pbuf, resid, rt, G, D, X, abuf, Y, R,
    dact, gsc, sel, selw, pb, s1, tb, s2,
    lsem, kvsem, wdss, wdrs, ddss, ddrs, tps, tpr, rts, rtr,
    gss, grs, gds, gdr, zs, zr, xds, xdr, as_, ar, das, dar, ys, yr,
    r1s, r1r, r2s, r2r,
):
    c = lax.axis_index("tp")
    ep = lax.axis_index("ep")
    z = ep // 16
    p0 = ep % 16
    y = p0 // 4
    x = p0 % 4
    sa = 1 + 3 * c
    sb = 4 - 3 * c
    a = x * (1 - c) + y * c
    b = y * (1 - c) + x * c
    zb = z * 16
    half = pl.ds(pl.multiple_of(c * HALF, HALF), HALF)
    other = 1 - c

    def local(src, dst, sem):
        return pltpu.make_async_copy(src, dst, sem)

    def remote(src, dst, ssem, rsem, **dev):
        return pltpu.make_async_remote_copy(
            src_ref=src, dst_ref=dst, send_sem=ssem, recv_sem=rsem,
            device_id=dev, device_id_type=pl.DeviceIdType.MESH,
        )

    def pidx(aa, bb):
        return aa * sa + bb * sb

    first = [
        local(wq_h, wq, lsem.at[0]),
        local(wk_h, wk, lsem.at[1]),
        local(wv_h, wv, lsem.at[2]),
    ]
    for cp in first:
        cp.start()

    def kv(g):
        rows = pl.ds(g * GRP, GRP)
        return (
            local(kc_h.at[rows], kb.at[rows], kvsem.at[0, g]),
            local(vc_h.at[rows], vb.at[rows], kvsem.at[1, g]),
        )

    own_w = local(wd_h, wdg.at[:, z], lsem.at[3])
    own_d = local(dd_h, ddg.at[:, z], lsem.at[4])
    own_w.start()
    own_d.start()

    @pl.loop(0, NGRP)
    def _(g):
        for cp in kv(g):
            cp.start()

    later = [
        local(wo_h, wo, lsem.at[5]),
        local(eg_h.at[0], eg, lsem.at[6]),
        local(eu_h.at[0], eu, lsem.at[7]),
        local(ed_h.at[0], ed, lsem.at[8]),
    ]
    for cp in later:
        cp.start()

    barrier = pltpu.get_barrier_semaphore()
    for k in range(1, 16):
        dest = zb + ((y + k // 4) % 4) * 4 + (x + k % 4) % 4
        pl.semaphore_signal(barrier, inc=1, device_id={"ep": dest}, device_id_type=pl.DeviceIdType.MESH)
    for k in range(1, 4):
        dest = ((z + k) % 4) * 16 + p0
        pl.semaphore_signal(barrier, inc=1, device_id={"ep": dest}, device_id_type=pl.DeviceIdType.MESH)
    pl.semaphore_signal(barrier, inc=1, device_id={"tp": other}, device_id_type=pl.DeviceIdType.MESH)
    pl.semaphore_wait(barrier, 19)

    def rt_copy(k):
        dest = zb + ((y + k // 4) % 4) * 4 + (x + k % 4) % 4
        return remote(route, rt.at[p0], rts.at[k], rtr.at[k], ep=dest)

    for k in range(1, 16):
        rt_copy(k).start()
    rt[p0] = route[...]

    own_w.wait()
    own_d.wait()

    def w_copy(k):
        dest = ((z + k) % 4) * 16 + p0
        return (
            remote(wdg.at[:, z], wdg.at[:, z], wdss.at[k], wdrs.at[k], ep=dest),
            remote(ddg.at[:, z], ddg.at[:, z], ddss.at[k], ddrs.at[k], ep=dest),
        )

    for k in (1, 3, 2):
        for cp in w_copy(k):
            cp.start()

    h = hid[...].astype(F32)
    normed = (h * lax.rsqrt(jnp.mean(h * h, axis=-1, keepdims=True) + EPS) * again[...]).astype(BF)
    cos = trig[0]
    sin = trig[1]
    low = (lax.broadcasted_iota(jnp.int32, (ROWS, 128), 1) & 63) < 32

    def rotated(v):
        turned = jnp.where(low, pltpu.roll(v, 96, 1), pltpu.roll(v, 32, 1))
        return (v * cos + turned * sin).astype(BF)

    for cp in first:
        cp.wait()
    new_k = rotated(dot(normed, wk[...]))
    new_v = dot(normed, wv[...]).astype(BF)
    nk[...] = new_k
    nv[...] = new_v
    kn[...] = new_k.astype(F32)
    vn[...] = new_v.astype(F32)
    q = dot(normed, wq[...])
    for i in range(8):
        qs[:, i, :] = rotated(q[:, i * 128 : (i + 1) * 128]).astype(F32) * 0.125

    lam_col = jnp.zeros((8, 128), F32)
    rows8 = lax.broadcasted_iota(jnp.int32, (8, 128), 0)
    for i in range(8):
        lam_col = jnp.where(rows8 == i, lam[i], lam_col)
    left = lax.broadcasted_iota(jnp.int32, (8, 128), 1) < 64
    last16 = lax.broadcasted_iota(jnp.int32, (16, 128), 0) == 15
    places = lax.broadcasted_iota(jnp.int32, (16, CACHE), 1)
    gain = hgain[...]

    @pl.loop(0, NGRP)
    def _(g):
        for cp in kv(g):
            cp.wait()
        for i in range(GRP):
            s = g * GRP + i
            tail = pl.ds(CACHE - 16, 16)
            kb[s, tail, :] = jnp.where(
                last16, jnp.broadcast_to(kn[pl.ds(s, 1), :], (16, 128)), kb[s, tail, :].astype(F32)
            ).astype(BF)
            vb[s, tail, :] = jnp.where(
                last16, jnp.broadcast_to(vn[pl.ds(s, 1), :], (16, 128)), vb[s, tail, :].astype(F32)
            ).astype(BF)
            qv = qs[s]
            q2 = jnp.concatenate(
                [jnp.where(left, qv, 0.0), jnp.where(left, 0.0, qv)], axis=0
            ).astype(BF)
            scores = dot_nt(q2, kb[s])
            usable = (places < plen[s]) | (places == CACHE - 1)
            scores = jnp.where(usable, scores, -jnp.inf)
            peak = jnp.max(scores, axis=-1, keepdims=True)
            weights = jnp.exp(scores - peak)
            total = jnp.sum(weights, axis=-1, keepdims=True)
            mapped = dot(weights.astype(BF), vb[s]) / total
            mix = mapped[0:8] - lam_col * mapped[8:16]
            ho[s] = mix * lax.rsqrt(jnp.mean(mix * mix, axis=-1, keepdims=True) + EPS) * gain

    later[0].wait()
    head_out = jnp.concatenate([ho[:, i, :].astype(BF) for i in range(8)], axis=1)
    pbuf[0] = dot(head_out, wo[...]).astype(BF)
    tp_copy = remote(pbuf.at[0], pbuf.at[1], tps, tpr, tp=other)
    tp_copy.start()
    tp_copy.wait()
    attn_out = (pbuf[0].astype(F32) + pbuf[1].astype(F32)).astype(BF)
    res = hid[...].astype(F32) + attn_out.astype(F32)
    resid[...] = res
    G[p0] = (
        res * lax.rsqrt(jnp.mean(res * res, axis=-1, keepdims=True) + EPS) * fgain[...]
    ).astype(BF)

    def g_copy(ka, kb_, da, db):
        src = pidx((a + 4 - ka) % 4, (b + 4 - kb_) % 4)
        dest = zb + pidx((a + da) % 4, (b + db) % 4)
        i = (ka + da) * 4 + kb_ + db
        return remote(
            G.at[src, :, half], G.at[src, :, half], gss.at[i], grs.at[i], ep=dest
        )

    def g_wait(ka, kb_):
        i = ka * 4 + kb_
        src = pidx((a + 4 - ka) % 4, (b + 4 - kb_) % 4)
        remote(
            G.at[src, :, half], G.at[src, :, half], gss.at[i], grs.at[i], tp=other
        ).wait_recv()

    def g_share(ka, kb_):
        src = pidx((a + 4 - ka) % 4, (b + 4 - kb_) % 4)
        i = ka * sa + kb_ * sb
        return remote(
            G.at[src, :, half], G.at[src, :, half], gds.at[i], gdr.at[i], tp=other
        )

    for k in (1, 3, 2):
        g_copy(0, 0, k, 0).start()
        g_copy(0, 0, 0, k).start()
    for k in range(1, 16):
        src = ((y + 4 - k // 4) % 4) * 4 + (x + 4 - k % 4) % 4
        remote(route, rt.at[src], rts.at[k], rtr.at[k], tp=other).wait_recv()
    facts = jnp.concatenate(
        [rt[4 * i] + rt[4 * i + 1] + rt[4 * i + 2] + rt[4 * i + 3] for i in range(4)], axis=1
    )
    row = lax.broadcasted_iota(jnp.int32, (256, 512), 0)
    token = lax.broadcasted_iota(jnp.int32, (256, 512), 1)
    target = ((((row >> 6) * 16 + p0) >> 1) * 4 + (row & 3)).astype(F32)
    mine = ((row >> 2) & 15) == (token >> 5)
    hit0 = mine & (facts[0:1] == target)
    hit1 = mine & (facts[1:2] == target)
    sel[...] = jnp.where(hit0 | hit1, 1.0, 0.0).astype(BF)
    selw[...] = (jnp.where(hit0, facts[2:3], 0.0) + jnp.where(hit1, facts[3:4], 0.0)).astype(BF)

    for ka in (1, 3, 2):
        g_wait(ka, 0)
        for k in (1, 3, 2):
            g_copy(ka, 0, 0, k).start()
        g_share(ka, 0).start()
    for ka in (0, 1, 3, 2):
        for kb_ in (1, 3, 2):
            g_wait(ka, kb_)
            g_share(ka, kb_).start()

    D[...] = dot(sel[...], G[:, :, half].reshape(512, HALF)).astype(BF).reshape(4, 64, HALF)

    def z_copy(k):
        to = (z + k) % 4
        return remote(D.at[to], X.at[z, :, half], zs.at[k], zr.at[k], ep=to * 16 + p0)

    def x_share(k):
        src = (z + 4 - k) % 4
        return remote(X.at[src, :, half], X.at[src, :, half], xds.at[k], xdr.at[k], tp=other)

    for k in (1, 3, 2):
        z_copy(k).start()
    X[z, :, half] = D[z]
    x_share(0).start()

    for k in range(1, 16):
        src = ((y + 4 - k // 4) % 4) * 4 + (x + 4 - k % 4) % 4
        oh = pl.ds(pl.multiple_of(other * HALF, HALF), HALF)
        remote(G.at[src, :, oh], G.at[src, :, oh], gds.at[k], gdr.at[k], tp=other).wait_recv()
    for k in range(1, 4):
        src = (z + 4 - k) % 4
        remote(wdg.at[:, src], wdg.at[:, src], wdss.at[k], wdrs.at[k], tp=other).wait_recv()
        remote(ddg.at[:, src], ddg.at[:, src], ddss.at[k], ddrs.at[k], tp=other).wait_recv()

    @pl.loop(0, 4)
    def _(i):
        tokens = G[pl.ds(i * 4, 4)].reshape(128, WIDTH)
        pre_gate = dot_nt(tokens, wdg[0].reshape(192, WIDTH))
        pre_up = dot_nt(tokens, wdg[1].reshape(192, WIDTH))
        act = pre_gate / (1.0 + jnp.exp(-pre_gate)) * pre_up
        dact[c, pl.ds(i * 128, 128), :] = jnp.concatenate(
            [act, jnp.zeros((128, 64), F32)], axis=1
        ).astype(BF)
        mix_gate = (1.0 / (1.0 + jnp.exp(-pre_gate[:, 44:45]))).astype(BF).astype(F32)
        gsc[pl.ds(i * 128, 128), :] = jnp.broadcast_to(mix_gate, (128, 128))

    act_copy = remote(dact.at[c], dact.at[c], das, dar, tp=other)
    act_copy.start()

    for k in (1, 3, 2):
        src = (z + 4 - k) % 4
        remote(D.at[0], X.at[src, :, half], zs.at[k], zr.at[k], tp=other).wait_recv()
        x_share(k).start()
    for cp in later[1:]:
        cp.wait()
    for k in (0, 1, 3, 2):
        src = (z + 4 - k) % 4
        oh = pl.ds(pl.multiple_of(other * HALF, HALF), HALF)
        remote(X.at[src, :, oh], X.at[src, :, oh], xds.at[k], xdr.at[k], tp=other).wait_recv()
    rows_in = X[...].reshape(256, WIDTH)
    gate_pre = dot(rows_in, eg[...])
    up_pre = dot(rows_in, eu[...])
    inner = gate_pre / (1.0 + jnp.exp(-gate_pre)) * up_pre
    abuf[c] = jnp.concatenate([inner, jnp.zeros((256, 32), F32)], axis=1).astype(BF)
    a_copy = remote(abuf.at[c], abuf.at[c], as_, ar, tp=other)
    a_copy.start()
    remote(abuf.at[other], abuf.at[other], as_, ar, tp=other).wait_recv()
    Y[...] = (
        dot(abuf[0][:, :352], ed[0:352, :]) + dot(abuf[1][:, :352], ed[352:704, :])
    ).astype(BF).reshape(4, 64, HALF)

    def y_copy(k):
        to = (z + k) % 4
        return remote(Y.at[to], R.at[z], ys.at[k], yr.at[k], ep=to * 16 + p0)

    for k in (1, 3, 2):
        y_copy(k).start()
    R[z] = Y[z]
    remote(dact.at[other], dact.at[other], das, dar, tp=other).wait_recv()
    for k in (1, 3, 2):
        src = (z + 4 - k) % 4
        remote(Y.at[0], R.at[src], ys.at[k], yr.at[k], tp=other).wait_recv()

    @pl.loop(0, 4)
    def _(i):
        rows = pl.ds(pl.multiple_of(i * 128, 128), 128)
        part = dot(dact[0, rows, :][:, :192], ddg[0].reshape(192, HALF)) + dot(
            dact[1, rows, :][:, :192], ddg[1].reshape(192, HALF)
        )
        part = part * gsc[rows, 0:1] + dot_tn(selw[:, rows], R[...].reshape(256, HALF))
        part = part.astype(BF).reshape(4, ROWS, HALF)
        for j in range(4):
            pb[i * sb + j * sa] = part[j]

    def r1_copy(k):
        to = (b + k) % 4
        return remote(
            pb.at[pl.ds(to * 4, 4)], s1.at[k - 1], r1s.at[k], r1r.at[k], ep=zb + pidx(a, to)
        )

    def r2_copy(k):
        to = (a + k) % 4
        return remote(tb.at[to], s2.at[k - 1], r2s.at[k], r2r.at[k], ep=zb + pidx(to, b))

    for k in (1, 3, 2):
        r1_copy(k).start()
    for k in (1, 3, 2):
        r1_copy(k).wait_recv()
    total1 = pb[pl.ds(b * 4, 4)].astype(F32)
    for k in range(3):
        total1 = total1 + s1[k].astype(F32)
    tb[...] = total1.astype(BF)
    for k in (1, 3, 2):
        r2_copy(k).start()
    for k in (1, 3, 2):
        r2_copy(k).wait_recv()
    final = tb[a].astype(F32)
    for k in range(3):
        final = final + s2[k].astype(F32)
    out[...] = (resid[:, half] + final).astype(BF)

    for k in range(1, 16):
        rt_copy(k).wait_send()
    for k in range(1, 4):
        for cp in w_copy(k):
            cp.wait_send()
        g_copy(0, 0, k, 0).wait_send()
        g_copy(0, 0, 0, k).wait_send()
        z_copy(k).wait_send()
        y_copy(k).wait_send()
        r1_copy(k).wait_send()
        r2_copy(k).wait_send()
    for ka in range(1, 4):
        for k in range(1, 4):
            g_copy(ka, 0, 0, k).wait_send()
    for ka in range(4):
        for kb_ in range(4):
            if ka or kb_:
                g_share(ka, kb_).wait_send()
    for k in range(4):
        x_share(k).wait_send()
    act_copy.wait_send()
    a_copy.wait_send()


def routing_block(route_ids, route_weights, x):
    same = route_ids[:, :, None, None] == route_ids[None, None, :, :]
    at = jnp.arange(ROWS)
    before = (at[None, :] < at[:, None])[:, None, :, None]
    rank = jnp.sum((same & before).astype(F32), axis=(2, 3))
    code = route_ids.astype(F32) * 4.0 + rank
    vals = jnp.concatenate([code, route_weights], axis=1)
    vals = jnp.concatenate([vals, jnp.zeros_like(vals)], axis=1)
    place = jnp.arange(128)[None, :] == (at + 32 * x)[:, None]
    return jnp.sum(jnp.where(place[:, None, :], vals[:, :, None], 0.0), axis=0)


def per_device(
    hidden_in, past_lengths, key_cache, value_cache, attn_gain, w_query, w_key, w_value,
    lambdas, head_gain, w_out, ffn_gain, route_ids, route_weights, expert_gate, expert_up,
    expert_down, gate_vector, dense_gate, dense_up, dense_down,
):
    lane = jnp.arange(128)
    inverse = ROPE_BASE ** (-(lane % 32).astype(F32) / 32)
    angles = past_lengths.astype(F32)[:, None] * inverse[None, :]
    sign = jnp.where(lane % 64 < 32, -1.0, 1.0)
    trig = jnp.stack([jnp.cos(angles), jnp.sin(angles) * sign])
    route = routing_block(route_ids, route_weights, lax.axis_index("ep") % 4)
    wd = jnp.stack(
        [
            jnp.concatenate([dense_gate.T, gate_vector[None], jnp.zeros((3, WIDTH), BF)]),
            jnp.concatenate([dense_up.T, jnp.zeros((4, WIDTH), BF)]),
        ]
    )
    dd = jnp.pad(dense_down.reshape(2, 44, HALF), ((0, 0), (0, 4), (0, 0)))
    vm = pl.BlockSpec(memory_space=pltpu.VMEM)
    sm = pl.BlockSpec(memory_space=pltpu.SMEM)
    hbm = pl.BlockSpec(memory_space=pl.ANY)
    V = pltpu.VMEM
    dma = pltpu.SemaphoreType.DMA
    scratch = [
        V((ROWS, CACHE, 128), BF), V((ROWS, CACHE, 128), BF),
        V((WIDTH, 1024), BF), V((WIDTH, 128), BF), V((WIDTH, 128), BF), V((1024, WIDTH), BF),
        V((WIDTH, 352), BF), V((WIDTH, 352), BF), V((704, HALF), BF),
        V((2, 4, 48, WIDTH), BF), V((2, 4, 48, HALF), BF),
        V((ROWS, 8, 128), F32), V((ROWS, 128), F32), V((ROWS, 128), F32), V((ROWS, 8, 128), F32),
        V((2, ROWS, WIDTH), BF), V((ROWS, WIDTH), F32), V((16, 8, 128), F32),
        V((16, ROWS, WIDTH), BF), V((4, 64, HALF), BF), V((4, 64, WIDTH), BF),
        V((2, 256, 384), BF), V((4, 64, HALF), BF), V((4, 64, HALF), BF),
        V((2, 512, 256), BF), V((512, 128), F32), V((256, 512), BF), V((256, 512), BF),
        V((16, ROWS, HALF), BF), V((3, 4, ROWS, HALF), BF), V((4, ROWS, HALF), BF),
        V((3, ROWS, HALF), BF),
        dma((9,)), dma((2, NGRP)), dma((4,)), dma((4,)), dma((4,)), dma((4,)), dma, dma,
        dma((16,)), dma((16,)),
        dma((16,)), dma((16,)), dma((16,)), dma((16,)), dma((4,)), dma((4,)), dma((4,)), dma((4,)),
        dma, dma, dma, dma, dma((4,)), dma((4,)),
        dma((4,)), dma((4,)), dma((4,)), dma((4,)),
    ]
    return pl.pallas_call(
        layer_kernel,
        name="layer",
        out_shape=(
            jax.ShapeDtypeStruct((ROWS, HALF), BF),
            jax.ShapeDtypeStruct((ROWS, 128), BF),
            jax.ShapeDtypeStruct((ROWS, 128), BF),
        ),
        in_specs=[vm, vm, sm, vm, sm, vm, vm, vm] + [hbm] * 11,
        out_specs=(vm, vm, vm),
        scratch_shapes=scratch,
        compiler_params=pltpu.CompilerParams(
            collective_id=0, has_side_effects=True, vmem_limit_bytes=66 * 1000 * 1000
        ),
    )(
        hidden_in, trig, past_lengths, attn_gain.reshape(1, WIDTH), lambdas,
        head_gain.reshape(1, 128), ffn_gain.reshape(1, WIDTH), route,
        key_cache, value_cache, w_query, w_key, w_value, w_out, expert_gate, expert_up,
        expert_down, wd, dd,
    )


def solution(mesh):
    return jax.shard_map(
        per_device,
        mesh=mesh,
        in_specs=(
            P("ep", None), P("ep"), P("ep", None, "tp"), P("ep", None, "tp"), P(),
            P(None, "tp"), P(None, "tp"), P(None, "tp"), P("tp"), P(), P("tp", None), P(),
            P("ep", None), P("ep", None), P("ep", None, "tp"), P("ep", None, "tp"),
            P("ep", None, "tp"), P(), P(None, ("ep", "tp")), P(None, ("ep", "tp")), P("ep", "tp"),
        ),
        out_specs=(P("ep", "tp"), P("ep", "tp"), P("ep", "tp")),
        check_vma=False,
    )
```

```python
import jax
import jax.numpy as jnp
import numpy as np
from jax import lax
from jax.experimental import pallas as pl
from jax.experimental.pallas import tpu as pltpu
from jax.sharding import PartitionSpec as P

EPS = 1e-05
ROPE_BASE = 10000.0
BF = jnp.bfloat16
F32 = jnp.float32
ROWS = 32
WIDTH = 2048
HALF = 1024
CACHE = 1024
GRP = 4
NGRP = ROWS // GRP
NT = (((1,), (1,)), ((), ()))
TN = (((0,), (0,)), ((), ()))


def dot(a, b):
    return jnp.dot(a, b, preferred_element_type=F32)


def dot_nt(a, b):
    return lax.dot_general(a, b, NT, preferred_element_type=F32)


def dot_tn(a, b):
    return lax.dot_general(a, b, TN, preferred_element_type=F32)


def layer_kernel(
    hid, freq, plen, prow, again, lam, hgain, fgain, ids, wts, gvec,
    kc_h, vc_h, wq_h, wk_h, wv_h, wo_h, eg_h, eu_h, ed_h, dg_h, du_h, dd_h,
    out,
    kb, vb, wq, wk, wv, wo, eg, eu, ed, dg, du, dtail,
    wdg, ddg, qs, kn, vn, ho, pbuf, resid, rt, G, D, X, tz, abuf, Y, R, ty,
    dact, gsc, sel, selw, pb, s1, t1, m1, tb, s2, t2, m2,
    lsem, kvsem, wss, wrs, tps, tpr, rts, rtr,
    gss, grs, gds, gdr, zs, zr, xds, xdr, as_, ar, das, dar, ys, yr,
    r1s, r1r, r2s, r2r,
):
    c = lax.axis_index("tp")
    ep = lax.axis_index("ep")
    z = ep // 16
    p0 = ep % 16
    y = p0 // 4
    x = p0 % 4
    sa = 1 + 3 * c
    sb = 4 - 3 * c
    a = x * (1 - c) + y * c
    b = y * (1 - c) + x * c
    zb = z * 16
    other = 1 - c
    half = pl.ds(pl.multiple_of(c * HALF, HALF), HALF)
    other_half = pl.ds(pl.multiple_of(other * HALF, HALF), HALF)

    def local(src, dst, sem):
        return pltpu.make_async_copy(src, dst, sem)

    def remote(src, dst, ssem, rsem, **dev):
        return pltpu.make_async_remote_copy(
            src_ref=src, dst_ref=dst, send_sem=ssem, recv_sem=rsem,
            device_id=dev, device_id_type=pl.DeviceIdType.MESH,
        )

    def pidx(aa, bb):
        return aa * sa + bb * sb

    def z_ep(step):
        return ((z + 4 + step) % 4) * 16 + p0

    def a_ep(step):
        return zb + pidx((a + 4 + step) % 4, b)

    def b_ep(step):
        return zb + pidx(a, (b + 4 + step) % 4)

    own_w = [
        local(dg_h, dg, lsem.at[3]),
        local(du_h, du, lsem.at[4]),
        local(dd_h.at[pl.ds(0, 48)], ddg.at[0, z], lsem.at[9]),
        local(dd_h.at[pl.ds(40, 48)], dtail, lsem.at[10]),
    ]
    first = [
        local(wk_h, wk, lsem.at[1]),
        local(wv_h, wv, lsem.at[2]),
        local(wq_h, wq, lsem.at[0]),
    ]
    for cp in own_w + first:
        cp.start()

    def kv(g):
        rows = pl.ds(g * GRP, GRP)
        return (
            local(kc_h.at[rows], kb.at[rows], kvsem.at[0, g]),
            local(vc_h.at[rows], vb.at[rows], kvsem.at[1, g]),
        )

    @pl.loop(0, NGRP)
    def _(g):
        for cp in kv(g):
            cp.start()

    later = [
        local(wo_h, wo, lsem.at[5]),
        local(eg_h.at[0], eg, lsem.at[6]),
        local(eu_h.at[0], eu, lsem.at[7]),
        local(ed_h.at[0], ed, lsem.at[8]),
    ]
    for cp in later:
        cp.start()

    barrier = pltpu.get_barrier_semaphore()
    for k in range(1, 16):
        dest = zb + ((y + k // 4) % 4) * 4 + (x + k % 4) % 4
        pl.semaphore_signal(barrier, inc=1, device_id={"ep": dest}, device_id_type=pl.DeviceIdType.MESH)
    for step in (1, -1):
        pl.semaphore_signal(barrier, inc=1, device_id={"ep": z_ep(step)}, device_id_type=pl.DeviceIdType.MESH)
    pl.semaphore_signal(barrier, inc=1, device_id={"tp": other}, device_id_type=pl.DeviceIdType.MESH)

    for cp in own_w:
        cp.wait()
    gv = gvec[...].astype(F32)
    gv = jnp.concatenate([gv[i : i + 1] for i in range(16)], axis=1)
    pad_row = lax.broadcasted_iota(jnp.int32, (4, WIDTH), 0)
    wdg[0, z, 0:44, :] = dg[...]
    wdg[0, z, 44:48, :] = jnp.where(pad_row == 0, gv, 0.0).astype(BF)
    wdg[1, z, 0:44, :] = du[...]
    wdg[1, z, 44:48, :] = jnp.zeros((4, WIDTH), BF)
    ddg[1, z] = pltpu.roll(dtail[...].astype(F32), 44, 0).astype(BF)

    at = lax.broadcasted_iota(jnp.int32, (ROWS, 128), 0)
    lane = lax.broadcasted_iota(jnp.int32, (ROWS, 128), 1)
    diag = at == lane
    shifted = at + 32 * x == lane

    def lanes(v, fill):
        return jnp.concatenate([v.astype(F32), jnp.full((v.shape[0], 128 - ROWS), fill, F32)], axis=1)

    def column(v):
        return jnp.sum(jnp.where(diag, v, 0.0), axis=1, keepdims=True)

    def moved(col):
        return jnp.sum(jnp.where(shifted, col, 0.0), axis=0, keepdims=True)

    id_rows = lanes(ids[...], -1.0)
    wt_rows = lanes(wts[...], 0.0)
    earlier = lane < at
    facts = []
    for k in range(2):
        col = column(id_rows[k : k + 1])
        same = jnp.where(id_rows[0:1] == col, 1.0, 0.0) + jnp.where(id_rows[1:2] == col, 1.0, 0.0)
        rank = jnp.sum(jnp.where(earlier, same, 0.0), axis=1, keepdims=True)
        facts.append(moved(col * 4.0 + rank))
    for k in range(2):
        facts.append(moved(column(wt_rows[k : k + 1])))
    facts.append(jnp.zeros((4, 128), F32))
    rt[p0] = jnp.concatenate(facts, axis=0)

    pl.semaphore_wait(barrier, 18)

    def rt_copy(k):
        dest = zb + ((y + k // 4) % 4) * 4 + (x + k % 4) % 4
        return remote(rt.at[p0], rt.at[p0], rts.at[k], rtr.at[k], ep=dest)

    for k in range(1, 16):
        rt_copy(k).start()

    def w_copy(i):
        block = (z + 4 + (0, 0, 0, 0, -1, 1, -1, 1)[i]) % 4
        ref = (
            wdg.at[:, block], wdg.at[:, block], ddg.at[:, block], ddg.at[:, block],
            wdg.at[0, block], wdg.at[1, block], ddg.at[0, block], ddg.at[1, block],
        )[i]
        return remote(ref, ref, wss.at[i], wrs.at[i], ep=z_ep((1, -1)[i % 2]))

    def w_wait(i):
        block = (z + 4 + (-1, 1, -1, 1, -2, 2, -2, 2)[i]) % 4
        ref = (
            wdg.at[:, block], wdg.at[:, block], ddg.at[:, block], ddg.at[:, block],
            wdg.at[0, block], wdg.at[1, block], ddg.at[0, block], ddg.at[1, block],
        )[i]
        remote(ref, ref, wss.at[i], wrs.at[i], tp=other).wait_recv()

    for i in range(4):
        w_copy(i).start()

    h = hid[...].astype(F32)
    normed = (h * lax.rsqrt(jnp.mean(h * h, axis=-1, keepdims=True) + EPS) * again[...]).astype(BF)
    angles = column(lanes(prow[...], 0.0)) * freq[...]
    cos = jnp.cos(angles)
    low = (lane & 63) < 32
    sin = jnp.sin(angles) * jnp.where(low, -1.0, 1.0)

    def rotated(v):
        turned = jnp.where(low, pltpu.roll(v, 96, 1), pltpu.roll(v, 32, 1))
        return (v * cos + turned * sin).astype(BF)

    for cp in first:
        cp.wait()
    new_k = rotated(dot(normed, wk[...]))
    new_v = dot(normed, wv[...]).astype(BF)
    out[:, HALF : HALF + 128] = new_k
    out[:, HALF + 128 : HALF + 256] = new_v
    kn[...] = new_k.astype(F32)
    vn[...] = new_v.astype(F32)
    q = dot(normed, wq[...])
    for i in range(8):
        qs[:, i, :] = rotated(q[:, i * 128 : (i + 1) * 128]).astype(F32) * 0.125

    lam_col = jnp.zeros((8, 128), F32)
    rows8 = lax.broadcasted_iota(jnp.int32, (8, 128), 0)
    for i in range(8):
        lam_col = jnp.where(rows8 == i, lam[i], lam_col)
    left = lax.broadcasted_iota(jnp.int32, (8, 128), 1) < 64
    last16 = lax.broadcasted_iota(jnp.int32, (16, 128), 0) == 15
    places = lax.broadcasted_iota(jnp.int32, (16, CACHE), 1)
    gain = hgain[...]

    def attend(lo, hi):
        @pl.loop(lo, hi)
        def _(g):
            for cp in kv(g):
                cp.wait()
            for i in range(GRP):
                s = g * GRP + i
                tail = pl.ds(CACHE - 16, 16)
                kb[s, tail, :] = jnp.where(
                    last16, jnp.broadcast_to(kn[pl.ds(s, 1), :], (16, 128)), kb[s, tail, :].astype(F32)
                ).astype(BF)
                vb[s, tail, :] = jnp.where(
                    last16, jnp.broadcast_to(vn[pl.ds(s, 1), :], (16, 128)), vb[s, tail, :].astype(F32)
                ).astype(BF)
                qv = qs[s]
                q2 = jnp.concatenate(
                    [jnp.where(left, qv, 0.0), jnp.where(left, 0.0, qv)], axis=0
                ).astype(BF)
                scores = dot_nt(q2, kb[s])
                usable = (places < plen[s]) | (places == CACHE - 1)
                scores = jnp.where(usable, scores, -jnp.inf)
                peak = jnp.max(scores, axis=-1, keepdims=True)
                weights = jnp.exp(scores - peak)
                total = jnp.sum(weights, axis=-1, keepdims=True)
                mapped = dot(weights.astype(BF), vb[s]) / total
                mix = mapped[0:8] - lam_col * mapped[8:16]
                ho[s] = mix * lax.rsqrt(jnp.mean(mix * mix, axis=-1, keepdims=True) + EPS) * gain

    attend(0, NGRP)

    later[0].wait()
    head_out = jnp.concatenate([ho[:, i, :].astype(BF) for i in range(8)], axis=1)
    pbuf[0] = dot(head_out, wo[...]).astype(BF)
    tp_copy = remote(pbuf.at[0], pbuf.at[1], tps, tpr, tp=other)
    tp_copy.start()
    for i in range(4):
        w_wait(i)
        w_copy(4 + i).start()
    tp_copy.wait()
    attn_out = (pbuf[0].astype(F32) + pbuf[1].astype(F32)).astype(BF)
    res = hid[...].astype(F32) + attn_out.astype(F32)
    resid[...] = res
    G[p0] = (
        res * lax.rsqrt(jnp.mean(res * res, axis=-1, keepdims=True) + EPS) * fgain[...]
    ).astype(BF)

    JA = (0, -1, 1, 2)

    def g_block(ja, jb, rows=pl.ds(0, ROWS)):
        return G.at[pidx((a + 4 + ja) % 4, (b + 4 + jb) % 4), rows, half]

    lo16, hi16 = pl.ds(0, 16), pl.ds(16, 16)

    def g_copy(i):
        if i < 4:
            ref = (g_block(0, 0), g_block(0, 0), g_block(-1, 0, lo16), g_block(1, 0, hi16))[i]
            return remote(ref, ref, gss.at[i], grs.at[i], ep=a_ep((1, -1)[i % 2]))
        ja, k = JA[i // 4 - 1], i % 4
        ref = (g_block(ja, 0), g_block(ja, 0), g_block(ja, -1, lo16), g_block(ja, 1, hi16))[k]
        return remote(ref, ref, gss.at[i], grs.at[i], ep=b_ep((1, -1)[k % 2]))

    def g_wait(i):
        k = i % 4
        step, rows = ((-1, None), (1, None), (-2, lo16), (2, hi16))[k]
        rows = pl.ds(0, ROWS) if rows is None else rows
        ref = g_block(step, 0, rows) if i < 4 else g_block(JA[i // 4 - 1], step, rows)
        remote(ref, ref, gss.at[i], grs.at[i], tp=other).wait_recv()

    def g_share(ja, jb):
        i = ((4 - ja) % 4) * sa + ((4 - jb) % 4) * sb
        ref = g_block(ja, jb)
        return remote(ref, ref, gds.at[i], gdr.at[i], tp=other)

    for i in (0, 1, 4, 5):
        g_copy(i).start()

    for k in range(1, 16):
        src = ((y + 4 - k // 4) % 4) * 4 + (x + 4 - k % 4) % 4
        remote(rt.at[src], rt.at[src], rts.at[k], rtr.at[k], tp=other).wait_recv()
    facts = jnp.concatenate(
        [rt[4 * i] + rt[4 * i + 1] + rt[4 * i + 2] + rt[4 * i + 3] for i in range(4)], axis=1
    )
    row = lax.broadcasted_iota(jnp.int32, (256, 512), 0)
    token = lax.broadcasted_iota(jnp.int32, (256, 512), 1)
    target = ((((row >> 6) * 16 + p0) >> 1) * 4 + (row & 3)).astype(F32)
    mine = ((row >> 2) & 15) == (token >> 5)
    hit0 = mine & (facts[0:1] == target)
    hit1 = mine & (facts[1:2] == target)
    sel[...] = jnp.where(hit0 | hit1, 1.0, 0.0).astype(BF)
    selw[...] = (jnp.where(hit0, facts[2:3], 0.0) + jnp.where(hit1, facts[3:4], 0.0)).astype(BF)

    def b_first(j):
        for k in (0, 1):
            g_wait(4 + 4 * j + k)
            g_copy(6 + 4 * j + k).start()
            g_share(JA[j], (-1, 1)[k]).start()

    def b_last(j):
        g_wait(6 + 4 * j)
        g_wait(7 + 4 * j)
        g_share(JA[j], 2).start()

    for k in (0, 1):
        g_wait(k)
        g_copy(2 + k).start()
        g_copy(8 + 4 * k).start()
        g_copy(9 + 4 * k).start()
        g_share((-1, 1)[k], 0).start()
    b_first(0)
    g_wait(2)
    g_wait(3)
    g_copy(16).start()
    g_copy(17).start()
    g_share(2, 0).start()
    b_first(1)
    b_last(0)
    b_first(2)
    b_last(1)
    b_first(3)
    b_last(2)
    b_last(3)

    D[...] = dot(sel[...], G[:, :, half].reshape(512, HALF)).astype(BF).reshape(4, 64, HALF)
    lo32, hi32 = pl.ds(0, 32), pl.ds(32, 32)
    whole = pl.ds(0, 64)

    def x_at(step, rows=whole):
        return X.at[(z + 4 + step) % 4, rows, half]

    def r_at(step, rows=whole):
        return R.at[(z + 4 + step) % 4, rows]

    def ring_copy(i, src, at_, mid, ss, rs):
        def piece(step, rows=whole):
            return src.at[(z + 4 + step) % 4, rows]

        pairs = (
            (piece(2, lo32), mid.at[0]), (piece(2, hi32), mid.at[1]),
            (piece(1), at_(0)), (piece(-1), at_(0)),
            (mid.at[0], at_(-1, lo32)), (mid.at[1], at_(1, hi32)),
        )
        return remote(pairs[i][0], pairs[i][1], ss.at[i], rs.at[i], ep=z_ep((1, -1)[i % 2]))

    def ring_wait(i, at_, mid, ss, rs):
        ref = (mid.at[0], mid.at[1], at_(-1), at_(1), at_(-2, lo32), at_(2, hi32))[i]
        remote(ref, ref, ss.at[i], rs.at[i], tp=other).wait_recv()

    def z_copy(i):
        return ring_copy(i, D, x_at, tz, zs, zr)

    def z_wait(i):
        ring_wait(i, x_at, tz, zs, zr)

    def x_share(step):
        i = (4 - step) % 4
        ref = x_at(step)
        return remote(ref, ref, xds.at[i], xdr.at[i], tp=other)

    for i in range(4):
        z_copy(i).start()
    X[z, :, half] = D[z]
    x_share(0).start()

    for i in range(4, 8):
        w_wait(i)
    for k in range(1, 16):
        src = ((y + 4 - k // 4) % 4) * 4 + (x + 4 - k % 4) % 4
        ref = G.at[src, :, other_half]
        remote(ref, ref, gds.at[k], gdr.at[k], tp=other).wait_recv()

    def dense_rows(i):
        tokens = G[pl.ds(i * 4, 4)].reshape(128, WIDTH)
        pre_gate = dot_nt(tokens, wdg[0].reshape(192, WIDTH))
        pre_up = dot_nt(tokens, wdg[1].reshape(192, WIDTH))
        act = pre_gate / (1.0 + jnp.exp(-pre_gate)) * pre_up
        rows = pl.ds(pl.multiple_of(i * 128, 128), 128)
        dact[c, rows, :] = jnp.concatenate([act, jnp.zeros((128, 64), F32)], axis=1).astype(BF)
        mix_gate = (1.0 / (1.0 + jnp.exp(-pre_gate[:, 44:45]))).astype(BF).astype(F32)
        gsc[rows, :] = jnp.broadcast_to(mix_gate, (128, 128))

    for i in (0, 1):
        z_wait(i)
        z_copy(4 + i).start()
    for i in (2, 3):
        z_wait(i)
        x_share((-1, 1)[i - 2]).start()

    @pl.loop(0, 4)
    def _(i):
        dense_rows(i)

    act_copy = remote(dact.at[c], dact.at[c], das, dar, tp=other)
    act_copy.start()

    z_wait(4)
    z_wait(5)
    x_share(2).start()
    for cp in later[1:]:
        cp.wait()
    for step in (0, -1, 1, 2):
        ref = X.at[(z + 4 + step) % 4, :, other_half]
        i = (4 - step) % 4
        remote(ref, ref, xds.at[i], xdr.at[i], tp=other).wait_recv()
    rows_in = X[...].reshape(256, WIDTH)
    gate_pre = dot_nt(rows_in, eg[...])
    up_pre = dot_nt(rows_in, eu[...])
    inner = gate_pre / (1.0 + jnp.exp(-gate_pre)) * up_pre
    abuf[c] = jnp.concatenate([inner, jnp.zeros((256, 32), F32)], axis=1).astype(BF)
    a_copy = remote(abuf.at[c], abuf.at[c], as_, ar, tp=other)
    a_copy.start()
    remote(abuf.at[other], abuf.at[other], as_, ar, tp=other).wait_recv()
    Y[...] = (
        dot(abuf[0][:, :352], ed[0:352, :]) + dot(abuf[1][:, :352], ed[352:704, :])
    ).astype(BF).reshape(4, 64, HALF)

    def y_copy(i):
        return ring_copy(i, Y, r_at, ty, ys, yr)

    def y_wait(i):
        ring_wait(i, r_at, ty, ys, yr)

    for i in range(4):
        y_copy(i).start()
    R[z] = Y[z]
    for i in (0, 1):
        y_wait(i)
        y_copy(4 + i).start()
    remote(dact.at[other], dact.at[other], das, dar, tp=other).wait_recv()
    for i in (2, 3, 4, 5):
        y_wait(i)

    @pl.loop(0, 4)
    def _(i):
        rows = pl.ds(pl.multiple_of(i * 128, 128), 128)
        part = dot(dact[0, rows, :][:, :192], ddg[0].reshape(192, HALF)) + dot(
            dact[1, rows, :][:, :192], ddg[1].reshape(192, HALF)
        )
        part = part * gsc[rows, 0:1] + dot_tn(selw[:, rows], R[...].reshape(256, HALF))
        part = part.astype(BF).reshape(4, ROWS, HALF)
        for j in range(4):
            pb[i * sb + j * sa] = part[j]

    def sum_ring(block, arrive, passing, merged, dest, ss, rs, n):
        upper, lower = pl.ds(0, n), pl.ds(n, n)

        def copy(i):
            pairs = (
                (block(2, upper), passing.at[0]), (block(2, lower), passing.at[1]),
                (block(1, lower), arrive.at[0, lower]), (block(-1, upper), arrive.at[1, upper]),
                (merged.at[0], arrive.at[0, upper]), (merged.at[1], arrive.at[1, lower]),
            )
            return remote(pairs[i][0], pairs[i][1], ss.at[i], rs.at[i], ep=dest((1, -1)[i % 2]))

        def wait(i):
            ref = (
                passing.at[0], passing.at[1], arrive.at[0, lower], arrive.at[1, upper],
                arrive.at[0, upper], arrive.at[1, lower],
            )[i]
            remote(ref, ref, ss.at[i], rs.at[i], tp=other).wait_recv()

        for i in range(4):
            copy(i).start()
        for i in (0, 1):
            wait(i)
            mine_ = block((1, -1)[i], (upper, lower)[i])
            merged[i] = (mine_[...].astype(F32) + passing[i].astype(F32)).astype(BF)
            copy(4 + i).start()
        for i in range(2, 6):
            wait(i)
        return copy

    def b_block(step, part):
        return pb.at[pl.ds(((b + 4 + step) % 4) * 4 + part.start, part.size)]

    def a_block(step, part):
        return tb.at[(a + 4 + step) % 4, part]

    r1_copy = sum_ring(b_block, s1, t1, m1, b_ep, r1s, r1r, 2)
    tb[...] = (
        pb[pl.ds(b * 4, 4)].astype(F32) + s1[0].astype(F32) + s1[1].astype(F32)
    ).astype(BF)
    r2_copy = sum_ring(a_block, s2, t2, m2, a_ep, r2s, r2r, 16)
    out[:, :HALF] = (
        resid[:, half] + (tb[a].astype(F32) + s2[0].astype(F32) + s2[1].astype(F32))
    ).astype(BF)

    for k in range(1, 16):
        rt_copy(k).wait_send()
    for i in range(8):
        w_copy(i).wait_send()
    for i in range(20):
        g_copy(i).wait_send()
    for i in range(6):
        z_copy(i).wait_send()
        y_copy(i).wait_send()
        r1_copy(i).wait_send()
        r2_copy(i).wait_send()
    for ja in JA:
        for jb in JA:
            if ja or jb:
                g_share(ja, jb).wait_send()
    for step in JA:
        x_share(step).wait_send()
    act_copy.wait_send()
    a_copy.wait_send()


def split_kernel(both, out, nk, nv, sem):
    copies = [
        pltpu.make_async_copy(both.at[:, pl.ds(0, HALF)], out, sem.at[0]),
        pltpu.make_async_copy(both.at[:, pl.ds(HALF, 128)], nk, sem.at[1]),
        pltpu.make_async_copy(both.at[:, pl.ds(HALF + 128, 128)], nv, sem.at[2]),
    ]
    for cp in copies:
        cp.start()
    for cp in copies:
        cp.wait()


def per_device(
    hidden_in, past_lengths, key_cache, value_cache, attn_gain, w_query, w_key, w_value,
    lambdas, head_gain, w_out, ffn_gain, route_ids, route_weights, expert_gate, expert_up,
    expert_down, gate_vector, dense_gate, dense_up, dense_down,
):
    freq = np.power(np.float32(ROPE_BASE), -(np.arange(128) % 32).astype(np.float32) / np.float32(32))
    freq = jnp.asarray(freq.astype(np.float32)[None])
    vm = pl.BlockSpec(memory_space=pltpu.VMEM)
    sm = pl.BlockSpec(memory_space=pltpu.SMEM)
    hbm = pl.BlockSpec(memory_space=pl.ANY)
    V = pltpu.VMEM
    dma = pltpu.SemaphoreType.DMA
    scratch = [
        V((ROWS, CACHE, 128), BF), V((ROWS, CACHE, 128), BF),
        V((WIDTH, 1024), BF), V((WIDTH, 128), BF), V((WIDTH, 128), BF), V((1024, WIDTH), BF),
        V((352, WIDTH), BF), V((352, WIDTH), BF), V((704, HALF), BF),
        V((44, WIDTH), BF), V((44, WIDTH), BF), V((48, HALF), BF),
        V((2, 4, 48, WIDTH), BF), V((2, 4, 48, HALF), BF),
        V((ROWS, 8, 128), F32), V((ROWS, 128), F32), V((ROWS, 128), F32), V((ROWS, 8, 128), F32),
        V((2, ROWS, WIDTH), BF), V((ROWS, WIDTH), F32), V((16, 8, 128), F32),
        V((16, ROWS, WIDTH), BF), V((4, 64, HALF), BF), V((4, 64, WIDTH), BF), V((2, 32, HALF), BF),
        V((2, 256, 384), BF), V((4, 64, HALF), BF), V((4, 64, HALF), BF), V((2, 32, HALF), BF),
        V((2, 512, 256), BF), V((512, 128), F32), V((256, 512), BF), V((256, 512), BF),
        V((16, ROWS, HALF), BF), V((2, 4, ROWS, HALF), BF), V((2, 2, ROWS, HALF), BF),
        V((2, 2, ROWS, HALF), BF), V((4, ROWS, HALF), BF),
        V((2, ROWS, HALF), BF), V((2, 16, HALF), BF), V((2, 16, HALF), BF),
        dma((11,)), dma((2, NGRP)), dma((8,)), dma((8,)), dma, dma,
        dma((16,)), dma((16,)),
        dma((20,)), dma((20,)), dma((16,)), dma((16,)), dma((6,)), dma((6,)), dma((4,)), dma((4,)),
        dma, dma, dma, dma, dma((6,)), dma((6,)),
        dma((6,)), dma((6,)), dma((6,)), dma((6,)),
    ]
    both = pl.pallas_call(
        layer_kernel,
        name="layer",
        out_shape=jax.ShapeDtypeStruct((ROWS, HALF + 256), BF),
        in_specs=[vm, vm, sm, vm, vm, sm, vm, vm, vm, vm, vm] + [hbm] * 12,
        out_specs=vm,
        scratch_shapes=scratch,
        compiler_params=pltpu.CompilerParams(
            collective_id=0, has_side_effects=True, vmem_limit_bytes=66 * 1000 * 1000
        ),
    )(
        hidden_in, freq, past_lengths, past_lengths.reshape(1, ROWS), attn_gain.reshape(1, WIDTH),
        lambdas, head_gain.reshape(1, 128), ffn_gain.reshape(1, WIDTH), route_ids.T,
        route_weights.T, gate_vector.reshape(16, 128),
        key_cache, value_cache, w_query, w_key, w_value, w_out,
        expert_gate.swapaxes(1, 2), expert_up.swapaxes(1, 2), expert_down,
        dense_gate.T, dense_up.T, dense_down,
    )
    return pl.pallas_call(
        split_kernel,
        name="split",
        out_shape=(
            jax.ShapeDtypeStruct((ROWS, HALF), BF),
            jax.ShapeDtypeStruct((ROWS, 128), BF),
            jax.ShapeDtypeStruct((ROWS, 128), BF),
        ),
        in_specs=[hbm],
        out_specs=(hbm, hbm, hbm),
        scratch_shapes=[dma((3,))],
    )(both)


def solution(mesh):
    return jax.shard_map(
        per_device,
        mesh=mesh,
        in_specs=(
            P("ep", None), P("ep"), P("ep", None, "tp"), P("ep", None, "tp"), P(),
            P(None, "tp"), P(None, "tp"), P(None, "tp"), P("tp"), P(), P("tp", None), P(),
            P("ep", None), P("ep", None), P("ep", None, "tp"), P("ep", None, "tp"),
            P("ep", None, "tp"), P(), P(None, ("ep", "tp")), P(None, ("ep", "tp")), P("ep", "tp"),
        ),
        out_specs=(P("ep", "tp"), P("ep", "tp"), P("ep", "tp")),
        check_vma=False,
    )
```

```python
import jax
import jax.numpy as jnp
import numpy as np
from jax import lax
from jax.experimental import pallas as pl
from jax.experimental.pallas import tpu as pltpu
from jax.sharding import PartitionSpec as P

EPS = 1e-05
ROPE_BASE = 10000.0
BF = jnp.bfloat16
F32 = jnp.float32
ROWS = 32
WIDTH = 2048
HALF = 1024
CACHE = 1024
GRP = 4
NGRP = ROWS // GRP
AHEAD = 3
VMEM_BYTES = 66 * 1000 * 1000
NEAR = (1, 3, 2)
NT = (((1,), (1,)), ((), ()))
TN = (((0,), (0,)), ((), ()))


def dot(a, b):
    return jnp.dot(a, b, preferred_element_type=F32)


def dot_nt(a, b):
    return lax.dot_general(a, b, NT, preferred_element_type=F32)


def dot_tn(a, b):
    return lax.dot_general(a, b, TN, preferred_element_type=F32)


def layer_kernel(
    hid, freq, plen, prow, again, lam, hgain, fgain, ids, wts, gvec,
    kc_h, vc_h, wq_h, wk_h, wv_h, wo_h, eg_h, eu_h, ed_h, dg_h, du_h, dd_h,
    out,
    kb, vb, wq, wk, wv, wo, eg, eu, ed, dg, du, dtail,
    wdg, ddg, qs, kn, vn, ho, pbuf, resid, rt, G, D, X, Xo, abuf, Y, R,
    dact, gsc, sel, selw, pb, s1, tb, s2,
    lsem, kvsem, wss, wrs, tps, tpr, rts, rtr,
    gss, grs, gds, gdr, zs, zr, xds, xdr, as_, ar, das, dar, ys, yr,
    r1s, r1r, r2s, r2r,
):
    c = lax.axis_index("tp")
    ep = lax.axis_index("ep")
    z = ep // 16
    p0 = ep % 16
    y = p0 // 4
    x = p0 % 4
    sa = 1 + 3 * c
    sb = 4 - 3 * c
    a = x * (1 - c) + y * c
    b = y * (1 - c) + x * c
    zb = z * 16
    other = 1 - c
    half = pl.ds(pl.multiple_of(c * HALF, HALF), HALF)
    other_half = pl.ds(pl.multiple_of(other * HALF, HALF), HALF)

    def local(src, dst, sem):
        return pltpu.make_async_copy(src, dst, sem)

    def remote(src, dst, ssem, rsem, **dev):
        return pltpu.make_async_remote_copy(
            src_ref=src, dst_ref=dst, send_sem=ssem, recv_sem=rsem,
            device_id=dev, device_id_type=pl.DeviceIdType.MESH,
        )

    def pidx(aa, bb):
        return aa * sa + bb * sb

    def z_ep(step):
        return ((z + 4 + step) % 4) * 16 + p0

    own_w = [
        local(dg_h, dg, lsem.at[3]),
        local(du_h, du, lsem.at[4]),
        local(dd_h.at[pl.ds(0, 48)], ddg.at[0, z], lsem.at[9]),
        local(dd_h.at[pl.ds(40, 48)], dtail, lsem.at[10]),
    ]
    first = [
        local(wk_h, wk, lsem.at[1]),
        local(wv_h, wv, lsem.at[2]),
        local(wq_h, wq, lsem.at[0]),
    ]
    for cp in own_w + first:
        cp.start()

    def kv(g):
        rows = pl.ds(g * GRP, GRP)
        return (
            local(kc_h.at[rows], kb.at[rows], kvsem.at[0, g]),
            local(vc_h.at[rows], vb.at[rows], kvsem.at[1, g]),
        )

    for g in range(AHEAD):
        for cp in kv(g):
            cp.start()

    later = [
        local(wo_h, wo, lsem.at[5]),
        local(eg_h.at[0], eg, lsem.at[6]),
        local(eu_h.at[0], eu, lsem.at[7]),
        local(ed_h.at[0], ed, lsem.at[8]),
    ]

    barrier = pltpu.get_barrier_semaphore()
    for k in range(1, 16):
        dest = zb + ((y + k // 4) % 4) * 4 + (x + k % 4) % 4
        pl.semaphore_signal(barrier, inc=1, device_id={"ep": dest}, device_id_type=pl.DeviceIdType.MESH)
    for step in NEAR:
        pl.semaphore_signal(barrier, inc=1, device_id={"ep": z_ep(step)}, device_id_type=pl.DeviceIdType.MESH)
    pl.semaphore_signal(barrier, inc=1, device_id={"tp": other}, device_id_type=pl.DeviceIdType.MESH)

    for cp in own_w:
        cp.wait()
    gv = gvec[...].astype(F32)
    gv = jnp.concatenate([gv[i : i + 1] for i in range(16)], axis=1)
    pad_row = lax.broadcasted_iota(jnp.int32, (4, WIDTH), 0)
    wdg[0, z, 0:44, :] = dg[...]
    wdg[0, z, 44:48, :] = jnp.where(pad_row == 0, gv, 0.0).astype(BF)
    wdg[1, z, 0:44, :] = du[...]
    wdg[1, z, 44:48, :] = jnp.zeros((4, WIDTH), BF)
    ddg[1, z] = pltpu.roll(dtail[...].astype(F32), 44, 0).astype(BF)

    at = lax.broadcasted_iota(jnp.int32, (ROWS, 128), 0)
    lane = lax.broadcasted_iota(jnp.int32, (ROWS, 128), 1)
    diag = at == lane
    shifted = at + 32 * a == lane

    def lanes(v, fill):
        return jnp.concatenate([v.astype(F32), jnp.full((v.shape[0], 128 - ROWS), fill, F32)], axis=1)

    def column(v):
        return jnp.sum(jnp.where(diag, v, 0.0), axis=1, keepdims=True)

    def moved(col):
        return jnp.sum(jnp.where(shifted, col, 0.0), axis=0, keepdims=True)

    id_rows = lanes(ids[...], -1.0)
    wt_rows = lanes(wts[...], 0.0)
    earlier = lane < at
    facts = []
    for k in range(2):
        col = column(id_rows[k : k + 1])
        same = jnp.where(id_rows[0:1] == col, 1.0, 0.0) + jnp.where(id_rows[1:2] == col, 1.0, 0.0)
        rank = jnp.sum(jnp.where(earlier, same, 0.0), axis=1, keepdims=True)
        facts.append(moved(col * 4.0 + rank))
    for k in range(2):
        facts.append(moved(column(wt_rows[k : k + 1])))
    facts.append(jnp.zeros((4, 128), F32))
    rt[p0] = jnp.concatenate(facts, axis=0)

    pl.semaphore_wait(barrier, 19)

    def rt_copy(k):
        dest = zb + ((y + k // 4) % 4) * 4 + (x + k % 4) % 4
        return remote(rt.at[p0], rt.at[p0], rts.at[k], rtr.at[k], ep=dest)

    for k in range(1, 16):
        rt_copy(k).start()

    def w_copy(i):
        block = (z + 4 + (0, 0, 0, 0, -1, 1, -1, 1)[i]) % 4
        ref = (
            wdg.at[:, block], wdg.at[:, block], ddg.at[:, block], ddg.at[:, block],
            wdg.at[0, block], wdg.at[1, block], ddg.at[0, block], ddg.at[1, block],
        )[i]
        return remote(ref, ref, wss.at[i], wrs.at[i], ep=z_ep((1, -1)[i % 2]))

    def w_wait(i):
        block = (z + 4 + (-1, 1, -1, 1, -2, 2, -2, 2)[i]) % 4
        ref = (
            wdg.at[:, block], wdg.at[:, block], ddg.at[:, block], ddg.at[:, block],
            wdg.at[0, block], wdg.at[1, block], ddg.at[0, block], ddg.at[1, block],
        )[i]
        remote(ref, ref, wss.at[i], wrs.at[i], tp=other).wait_recv()

    for i in (2, 3, 0, 1):
        w_copy(i).start()

    h = hid[...].astype(F32)
    normed = (h * lax.rsqrt(jnp.mean(h * h, axis=-1, keepdims=True) + EPS) * again[...]).astype(BF)
    angles = column(lanes(prow[...], 0.0)) * freq[...]
    cos = jnp.cos(angles)
    low = (lane & 63) < 32
    sin = jnp.sin(angles) * jnp.where(low, -1.0, 1.0)

    def rotated(v):
        turned = jnp.where(low, pltpu.roll(v, 96, 1), pltpu.roll(v, 32, 1))
        return (v * cos + turned * sin).astype(BF)

    for cp in first:
        cp.wait()
    new_k = rotated(dot(normed, wk[...]))
    new_v = dot(normed, wv[...]).astype(BF)
    out[:, HALF : HALF + 128] = new_k
    out[:, HALF + 128 : HALF + 256] = new_v
    kn[...] = new_k.astype(F32)
    vn[...] = new_v.astype(F32)
    q = dot(normed, wq[...])
    for i in range(8):
        qs[:, i, :] = rotated(q[:, i * 128 : (i + 1) * 128]).astype(F32) * 0.125

    lam_col = jnp.zeros((8, 128), F32)
    rows8 = lax.broadcasted_iota(jnp.int32, (8, 128), 0)
    for i in range(8):
        lam_col = jnp.where(rows8 == i, lam[i], lam_col)
    left = lax.broadcasted_iota(jnp.int32, (8, 128), 1) < 64
    last16 = lax.broadcasted_iota(jnp.int32, (16, 128), 0) == 15
    places = lax.broadcasted_iota(jnp.int32, (16, CACHE), 1)
    gain = hgain[...]

    @pl.loop(0, NGRP)
    def _(g):
        for cp in kv(g):
            cp.wait()

        @pl.when(g + AHEAD < NGRP)
        def _():
            for cp in kv(g + AHEAD):
                cp.start()

        @pl.when(g + AHEAD == NGRP)
        def _():
            later[0].start()

        for i in range(GRP):
            s = g * GRP + i
            tail = pl.ds(CACHE - 16, 16)
            kb[s, tail, :] = jnp.where(
                last16, jnp.broadcast_to(kn[pl.ds(s, 1), :], (16, 128)), kb[s, tail, :].astype(F32)
            ).astype(BF)
            vb[s, tail, :] = jnp.where(
                last16, jnp.broadcast_to(vn[pl.ds(s, 1), :], (16, 128)), vb[s, tail, :].astype(F32)
            ).astype(BF)
            qv = qs[s]
            q2 = jnp.concatenate(
                [jnp.where(left, qv, 0.0), jnp.where(left, 0.0, qv)], axis=0
            ).astype(BF)
            scores = dot_nt(q2, kb[s])
            usable = (places < plen[s]) | (places == CACHE - 1)
            scores = jnp.where(usable, scores, -jnp.inf)
            peak = jnp.max(scores, axis=-1, keepdims=True)
            weights = jnp.exp(scores - peak)
            total = jnp.sum(weights, axis=-1, keepdims=True)
            mapped = dot(weights.astype(BF), vb[s]) / total
            mix = mapped[0:8] - lam_col * mapped[8:16]
            ho[s] = mix * lax.rsqrt(jnp.mean(mix * mix, axis=-1, keepdims=True) + EPS) * gain

    for cp in later[1:]:
        cp.start()
    later[0].wait()
    head_out = jnp.concatenate([ho[:, i, :].astype(BF) for i in range(8)], axis=1)
    pbuf[0] = dot(head_out, wo[...]).astype(BF)
    tp_copy = remote(pbuf.at[0], pbuf.at[1], tps, tpr, tp=other)
    tp_copy.start()
    tp_copy.wait()
    attn_out = (pbuf[0].astype(F32) + pbuf[1].astype(F32)).astype(BF)
    res = hid[...].astype(F32) + attn_out.astype(F32)
    resid[...] = res
    G[b * 4 + a] = (
        res * lax.rsqrt(jnp.mean(res * res, axis=-1, keepdims=True) + EPS) * fgain[...]
    ).astype(BF)

    def g_copy(ka, kb_, da, db):
        src = ((b + 4 - kb_) % 4) * 4 + (a + 4 - ka) % 4
        dest = zb + pidx((a + da) % 4, (b + db) % 4)
        i = (ka + da) * 4 + kb_ + db
        ref = G.at[src, :, half]
        return remote(ref, ref, gss.at[i], grs.at[i], ep=dest)

    def g_share(ka, kb_):
        aa, bb = (a + 4 - ka) % 4, (b + 4 - kb_) % 4
        i = kb_ * 4 + ka
        return remote(
            G.at[bb * 4 + aa, :, half], G.at[aa * 4 + bb, :, half], gds.at[i], gdr.at[i], tp=other
        )

    def g_arrive(ka, kb_):
        i = ka * 4 + kb_
        ref = G.at[((b + 4 - kb_) % 4) * 4 + (a + 4 - ka) % 4, :, half]
        remote(ref, ref, gss.at[i], grs.at[i], tp=other).wait_recv()
        g_share(ka, kb_).start()

    for k in NEAR:
        g_copy(0, 0, k, 0).start()
        g_copy(0, 0, 0, k).start()

    for i in (2, 3):
        w_wait(i)
        w_copy(4 + i).start()

    for k in range(1, 16):
        src = ((y + 4 - k // 4) % 4) * 4 + (x + 4 - k % 4) % 4
        remote(rt.at[src], rt.at[src], rts.at[k], rtr.at[k], tp=other).wait_recv()
    row = lax.broadcasted_iota(jnp.int32, (64, 128), 0)
    token = lax.broadcasted_iota(jnp.int32, (64, 128), 1)
    target = ((((row >> 4) * 16 + p0) >> 1) * 4 + (row & 3)).astype(F32)
    mine = ((row >> 2) & 3) == (token >> 5)
    for i in range(4):
        facts = rt[pidx(0, i)] + rt[pidx(1, i)] + rt[pidx(2, i)] + rt[pidx(3, i)]
        hit0 = mine & (facts[0:1] == target)
        hit1 = mine & (facts[1:2] == target)
        sel[i] = jnp.where(hit0 | hit1, 1.0, 0.0).astype(BF)
        selw[i] = (jnp.where(hit0, facts[2:3], 0.0) + jnp.where(hit1, facts[3:4], 0.0)).astype(BF)

    def z_copy(k, kb_):
        to, g = (z + k) % 4, (b + 4 - kb_) % 4
        return remote(D.at[to, g], X.at[z, g], zs.at[k, kb_], zr.at[k, kb_], ep=to * 16 + p0)

    def select(kb_):
        g = (b + 4 - kb_) % 4
        rows_ = dot(sel[g], G[pl.ds(g * 4, 4), :, half].reshape(128, HALF))
        rows_ = rows_.astype(BF).reshape(4, 16, HALF)
        for i in range(4):
            D[i, g] = rows_[i]
        for k in NEAR:
            z_copy(k, kb_).start()

    for ka in NEAR:
        g_arrive(ka, 0)
    for k in NEAR:
        for ka in NEAR:
            g_copy(ka, 0, 0, k).start()
    select(0)
    for k in NEAR:
        for ka in (0, 1, 3, 2):
            g_arrive(ka, k)
        select(k)
        if k == 1:
            for i in (0, 1):
                w_wait(i)
                w_copy(4 + i).start()
    X[z] = D[z]

    def x_share(k):
        src = (z + 4 - k) % 4
        return remote(X.at[src], Xo.at[src], xds.at[k], xdr.at[k], tp=other)

    x_share(0).start()

    for i in range(4, 8):
        w_wait(i)
    for ka in range(4):
        for kb_ in range(4):
            if ka or kb_:
                i = ka * 4 + kb_
                ref = G.at[((b + 4 - kb_) % 4) * 4 + (a + 4 - ka) % 4, :, other_half]
                remote(ref, ref, gds.at[i], gdr.at[i], tp=other).wait_recv()

    @pl.loop(0, 4)
    def _(g):
        tokens = G[pl.ds(g * 4, 4)].reshape(128, WIDTH)
        pre_gate = dot_nt(tokens, wdg[0].reshape(192, WIDTH))
        pre_up = dot_nt(tokens, wdg[1].reshape(192, WIDTH))
        act = pre_gate / (1.0 + jnp.exp(-pre_gate)) * pre_up
        act = jnp.concatenate([act, jnp.zeros((128, 64), F32)], axis=1).astype(BF)
        dact[0, pl.ds(g * 4, 4)] = act.reshape(4, ROWS, 256)
        mix_gate = (1.0 / (1.0 + jnp.exp(-pre_gate[:, 44:45]))).astype(BF).astype(F32)
        gsc[g] = jnp.broadcast_to(mix_gate, (128, 128))

    act_copy = remote(dact.at[0], dact.at[1], das, dar, tp=other)
    act_copy.start()

    for k in NEAR:
        src = (z + 4 - k) % 4
        for kb_ in (0, 1, 3, 2):
            ref = X.at[src, (b + 4 - kb_) % 4]
            remote(ref, ref, zs.at[k, kb_], zr.at[k, kb_], tp=other).wait_recv()
        x_share(k).start()
    for cp in later[1:]:
        cp.wait()
    rr = lax.broadcasted_iota(jnp.int32, (256, 256), 0)
    cc = lax.broadcasted_iota(jnp.int32, (256, 256), 1)
    swap = (rr & 195) + ((rr >> 2) & 12) + ((rr & 12) << 2) == cc
    swap = jnp.where(swap, 1.0, 0.0).astype(BF)
    own_rows = X[...].reshape(256, HALF)
    gate_pre = dot_nt(own_rows, eg[:, half])
    up_pre = dot_nt(own_rows, eu[:, half])
    for k in (0, 1, 3, 2):
        ref = Xo.at[(z + 4 - k) % 4]
        remote(ref, ref, xds.at[k], xdr.at[k], tp=other).wait_recv()
    rows_in = dot(swap, Xo[...].reshape(256, HALF)).astype(BF)
    gate_pre = gate_pre + dot_nt(rows_in, eg[:, other_half])
    up_pre = up_pre + dot_nt(rows_in, eu[:, other_half])
    inner = gate_pre / (1.0 + jnp.exp(-gate_pre)) * up_pre
    abuf[0] = jnp.concatenate([inner, jnp.zeros((256, 32), F32)], axis=1).astype(BF)
    a_copy = remote(abuf.at[0], abuf.at[1], as_, ar, tp=other)
    a_copy.start()
    own_ed = ed[pl.ds(pl.multiple_of(c * 352, 32), 352), :]
    other_ed = ed[pl.ds(pl.multiple_of(other * 352, 32), 352), :]
    down = dot(abuf[0][:, :352], own_ed)
    remote(abuf.at[0], abuf.at[1], as_, ar, tp=other).wait_recv()
    other_act = dot(swap, abuf[1]).astype(BF)
    down = down + dot(other_act[:, :352], other_ed)
    Y[...] = down.astype(BF).reshape(4, 4, 16, HALF)

    def y_copy(k, kb_):
        to, g = (z + k) % 4, (b + kb_) % 4
        return remote(Y.at[to, g], R.at[z, g], ys.at[k, kb_], yr.at[k, kb_], ep=to * 16 + p0)

    for kb_ in (1, 3, 2, 0):
        for k in NEAR:
            y_copy(k, kb_).start()
    R[z] = Y[z]
    remote(dact.at[0], dact.at[1], das, dar, tp=other).wait_recv()

    def r1_copy(k):
        to = (b + k) % 4
        return remote(pb.at[to], s1.at[k - 1], r1s.at[k], r1r.at[k], ep=zb + pidx(a, to))

    def r2_copy(k):
        to = (a + k) % 4
        return remote(tb.at[to], s2.at[k - 1], r2s.at[k], r2r.at[k], ep=zb + pidx(to, b))

    for kb_ in (1, 3, 2, 0):
        g = (b + kb_) % 4
        other_act = jnp.concatenate([dact[1, i * 4 + g] for i in range(4)], axis=0)
        part = dot(dact[0, pl.ds(g * 4, 4)].reshape(128, 256)[:, :192], ddg[c].reshape(192, HALF)) + dot(
            other_act[:, :192], ddg[other].reshape(192, HALF)
        )
        for k in NEAR:
            ref = R.at[(z + 4 - k) % 4, g]
            remote(ref, ref, ys.at[k, kb_], yr.at[k, kb_], tp=other).wait_recv()
        rows_back = jnp.concatenate([R[i, g] for i in range(4)], axis=0)
        part = part * gsc[g][:, 0:1] + dot_tn(selw[g], rows_back)
        pb[g] = part.astype(BF).reshape(4, ROWS, HALF)
        if kb_:
            r1_copy(kb_).start()
    for k in NEAR:
        r1_copy(k).wait_recv()
    tb[...] = (
        pb[b].astype(F32) + s1[0].astype(F32) + s1[1].astype(F32) + s1[2].astype(F32)
    ).astype(BF)
    for k in NEAR:
        r2_copy(k).start()
    for k in NEAR:
        r2_copy(k).wait_recv()
    final = tb[a].astype(F32) + s2[0].astype(F32) + s2[1].astype(F32) + s2[2].astype(F32)
    out[:, :HALF] = (resid[:, half] + final).astype(BF)

    for k in range(1, 16):
        rt_copy(k).wait_send()
    for i in range(8):
        w_copy(i).wait_send()
    for k in NEAR:
        g_copy(0, 0, k, 0).wait_send()
        g_copy(0, 0, 0, k).wait_send()
        r1_copy(k).wait_send()
        r2_copy(k).wait_send()
        for i in range(4):
            z_copy(k, i).wait_send()
            y_copy(k, i).wait_send()
            if i:
                g_copy(i, 0, 0, k).wait_send()
    for i in range(1, 16):
        g_share(i // 4, i % 4).wait_send()
    for k in range(4):
        x_share(k).wait_send()
    act_copy.wait_send()
    a_copy.wait_send()


def split_kernel(both, out, nk, nv, sem):
    copies = [
        pltpu.make_async_copy(both.at[:, pl.ds(0, HALF)], out, sem.at[0]),
        pltpu.make_async_copy(both.at[:, pl.ds(HALF, 128)], nk, sem.at[1]),
        pltpu.make_async_copy(both.at[:, pl.ds(HALF + 128, 128)], nv, sem.at[2]),
    ]
    for cp in copies:
        cp.start()
    for cp in copies:
        cp.wait()


def per_device(
    hidden_in, past_lengths, key_cache, value_cache, attn_gain, w_query, w_key, w_value,
    lambdas, head_gain, w_out, ffn_gain, route_ids, route_weights, expert_gate, expert_up,
    expert_down, gate_vector, dense_gate, dense_up, dense_down,
):
    freq = np.power(np.float32(ROPE_BASE), -(np.arange(128) % 32).astype(np.float32) / np.float32(32))
    freq = jnp.asarray(freq.astype(np.float32)[None])
    vm = pl.BlockSpec(memory_space=pltpu.VMEM)
    sm = pl.BlockSpec(memory_space=pltpu.SMEM)
    hbm = pl.BlockSpec(memory_space=pl.ANY)
    V = pltpu.VMEM
    dma = pltpu.SemaphoreType.DMA
    scratch = [
        V((ROWS, CACHE, 128), BF), V((ROWS, CACHE, 128), BF),
        V((WIDTH, 1024), BF), V((WIDTH, 128), BF), V((WIDTH, 128), BF), V((1024, WIDTH), BF),
        V((352, WIDTH), BF), V((352, WIDTH), BF), V((704, HALF), BF),
        V((44, WIDTH), BF), V((44, WIDTH), BF), V((48, HALF), BF),
        V((2, 4, 48, WIDTH), BF), V((2, 4, 48, HALF), BF),
        V((ROWS, 8, 128), F32), V((ROWS, 128), F32), V((ROWS, 128), F32), V((ROWS, 8, 128), F32),
        V((2, ROWS, WIDTH), BF), V((ROWS, WIDTH), F32), V((16, 8, 128), F32),
        V((16, ROWS, WIDTH), BF), V((4, 4, 16, HALF), BF), V((4, 4, 16, HALF), BF),
        V((4, 4, 16, HALF), BF), V((2, 256, 384), BF), V((4, 4, 16, HALF), BF),
        V((4, 4, 16, HALF), BF), V((2, 16, ROWS, 256), BF), V((4, 128, 128), F32),
        V((4, 64, 128), BF), V((4, 64, 128), BF), V((4, 4, ROWS, HALF), BF),
        V((3, 4, ROWS, HALF), BF), V((4, ROWS, HALF), BF), V((3, ROWS, HALF), BF),
        dma((11,)), dma((2, NGRP)), dma((8,)), dma((8,)), dma, dma,
        dma((16,)), dma((16,)),
        dma((16,)), dma((16,)), dma((16,)), dma((16,)), dma((4, 4)), dma((4, 4)), dma((4,)),
        dma((4,)), dma, dma, dma, dma, dma((4, 4)), dma((4, 4)),
        dma((4,)), dma((4,)), dma((4,)), dma((4,)),
    ]
    both = pl.pallas_call(
        layer_kernel,
        name="layer",
        out_shape=jax.ShapeDtypeStruct((ROWS, HALF + 256), BF),
        in_specs=[vm, vm, sm, vm, vm, sm, vm, vm, vm, vm, vm] + [hbm] * 12,
        out_specs=vm,
        scratch_shapes=scratch,
        compiler_params=pltpu.CompilerParams(
            collective_id=0, has_side_effects=True, vmem_limit_bytes=VMEM_BYTES
        ),
    )(
        hidden_in, freq, past_lengths, past_lengths.reshape(1, ROWS), attn_gain.reshape(1, WIDTH),
        lambdas, head_gain.reshape(1, 128), ffn_gain.reshape(1, WIDTH), route_ids.T,
        route_weights.T, gate_vector.reshape(16, 128),
        key_cache, value_cache, w_query, w_key, w_value, w_out,
        expert_gate.swapaxes(1, 2), expert_up.swapaxes(1, 2), expert_down,
        dense_gate.T, dense_up.T, dense_down,
    )
    return pl.pallas_call(
        split_kernel,
        name="split",
        out_shape=(
            jax.ShapeDtypeStruct((ROWS, HALF), BF),
            jax.ShapeDtypeStruct((ROWS, 128), BF),
            jax.ShapeDtypeStruct((ROWS, 128), BF),
        ),
        in_specs=[hbm],
        out_specs=(hbm, hbm, hbm),
        scratch_shapes=[dma((3,))],
        compiler_params=pltpu.CompilerParams(vmem_limit_bytes=1 << 20),
    )(both)


def solution(mesh):
    return jax.shard_map(
        per_device,
        mesh=mesh,
        in_specs=(
            P("ep", None), P("ep"), P("ep", None, "tp"), P("ep", None, "tp"), P(),
            P(None, "tp"), P(None, "tp"), P(None, "tp"), P("tp"), P(), P("tp", None), P(),
            P("ep", None), P("ep", None), P("ep", None, "tp"), P("ep", None, "tp"),
            P("ep", None, "tp"), P(), P(None, ("ep", "tp")), P(None, ("ep", "tp")), P("ep", "tp"),
        ),
        out_specs=(P("ep", "tp"), P("ep", "tp"), P("ep", "tp")),
        check_vma=False,
    )
```

```python
import jax
import jax.numpy as jnp
import numpy as np
from jax import lax
from jax.experimental import pallas as pl
from jax.experimental.pallas import tpu as pltpu
from jax.sharding import PartitionSpec as P

EPS = 1e-05
ROPE_BASE = 10000.0
BF = jnp.bfloat16
F32 = jnp.float32
ROWS = 32
WIDTH = 2048
HALF = 1024
CACHE = 1024
GRP = 4
NGRP = ROWS // GRP
AHEAD = 3
VMEM_BYTES = 66 * 1000 * 1000
NEAR = (1, 3, 2)
MATES = tuple((i // 4, i % 4) for i in (10, 6, 14, 9, 11, 2, 8, 5, 7, 13, 15, 1, 3, 4, 12))
NT = (((1,), (1,)), ((), ()))
TN = (((0,), (0,)), ((), ()))


def dot(a, b):
    return jnp.dot(a, b, preferred_element_type=F32)


def dot_nt(a, b):
    return lax.dot_general(a, b, NT, preferred_element_type=F32)


def dot_tn(a, b):
    return lax.dot_general(a, b, TN, preferred_element_type=F32)


def layer_kernel(
    hid, freq, plen, prow, again, lam, hgain, fgain, ids, wts, gvec,
    kc_h, vc_h, wq_h, wk_h, wv_h, wo_h, eg_h, eu_h, ed_h, dg_h, du_h, dd_h,
    out,
    kb, vb, wq, wk, wv, wo, eg, eu, ed, dg, du, dtail,
    wdg, ddg, qs, kn, vn, ho, pbuf, resid, rt, G, zg, D, X, Xo, abuf, Y, R, M, m_in,
    dact, gsc, sel, selw, pb, s1, tb, s2,
    lsem, kvsem, wss, wrs, tps, tpr, rts, rtr,
    gss, grs, gds, gdr, zs, zr, xs, xr, xds, xdr, as_, ar, das, dar, ys, yr,
    r1s, r1r, r2s, r2r, ms, mr,
):
    c = lax.axis_index("tp")
    ep = lax.axis_index("ep")
    z = ep // 16
    p0 = ep % 16
    y = p0 // 4
    x = p0 % 4
    sa = 1 + 3 * c
    sb = 4 - 3 * c
    a = x * (1 - c) + y * c
    b = y * (1 - c) + x * c
    zb = z * 16
    other = 1 - c
    half = pl.ds(pl.multiple_of(c * HALF, HALF), HALF)
    other_half = pl.ds(pl.multiple_of(other * HALF, HALF), HALF)

    def local(src, dst, sem):
        return pltpu.make_async_copy(src, dst, sem)

    def remote(src, dst, ssem, rsem, **dev):
        return pltpu.make_async_remote_copy(
            src_ref=src, dst_ref=dst, send_sem=ssem, recv_sem=rsem,
            device_id=dev, device_id_type=pl.DeviceIdType.MESH,
        )

    def pidx(aa, bb):
        return aa * sa + bb * sb

    def z_ep(step):
        return ((z + 4 + step) % 4) * 16 + p0

    own_w = [
        local(dg_h, dg, lsem.at[3]),
        local(du_h, du, lsem.at[4]),
        local(dd_h.at[pl.ds(0, 48)], ddg.at[0, z], lsem.at[9]),
        local(dd_h.at[pl.ds(40, 48)], dtail, lsem.at[10]),
    ]
    first = [
        local(wk_h, wk, lsem.at[1]),
        local(wv_h, wv, lsem.at[2]),
        local(wq_h, wq, lsem.at[0]),
    ]
    for cp in own_w + first:
        cp.start()

    def kv(g):
        rows = pl.ds(g * GRP, GRP)
        return (
            local(kc_h.at[rows], kb.at[rows], kvsem.at[0, g]),
            local(vc_h.at[rows], vb.at[rows], kvsem.at[1, g]),
        )

    for g in range(AHEAD):
        for cp in kv(g):
            cp.start()

    later = [
        local(wo_h, wo, lsem.at[5]),
        local(eg_h.at[0], eg, lsem.at[6]),
        local(eu_h.at[0], eu, lsem.at[7]),
        local(ed_h.at[0], ed, lsem.at[8]),
    ]

    barrier = pltpu.get_barrier_semaphore()
    for k in range(1, 16):
        dest = zb + ((y + k // 4) % 4) * 4 + (x + k % 4) % 4
        pl.semaphore_signal(barrier, inc=1, device_id={"ep": dest}, device_id_type=pl.DeviceIdType.MESH)
    for step in NEAR:
        pl.semaphore_signal(barrier, inc=1, device_id={"ep": z_ep(step)}, device_id_type=pl.DeviceIdType.MESH)
    pl.semaphore_signal(barrier, inc=1, device_id={"tp": other}, device_id_type=pl.DeviceIdType.MESH)

    for cp in own_w:
        cp.wait()
    gv = gvec[...].astype(F32)
    gv = jnp.concatenate([gv[i : i + 1] for i in range(16)], axis=1)
    pad_row = lax.broadcasted_iota(jnp.int32, (4, WIDTH), 0)
    wdg[0, z, 0:44, :] = dg[...]
    wdg[0, z, 44:48, :] = jnp.where(pad_row == 0, gv, 0.0).astype(BF)
    wdg[1, z, 0:44, :] = du[...]
    wdg[1, z, 44:48, :] = jnp.zeros((4, WIDTH), BF)
    ddg[1, z] = pltpu.roll(dtail[...].astype(F32), 44, 0).astype(BF)

    at = lax.broadcasted_iota(jnp.int32, (ROWS, 128), 0)
    lane = lax.broadcasted_iota(jnp.int32, (ROWS, 128), 1)
    diag = at == lane
    shifted = at + 32 * z == lane

    def lanes(v, fill):
        return jnp.concatenate([v.astype(F32), jnp.full((v.shape[0], 128 - ROWS), fill, F32)], axis=1)

    def column(v):
        return jnp.sum(jnp.where(diag, v, 0.0), axis=1, keepdims=True)

    def moved(col):
        return jnp.sum(jnp.where(shifted, col, 0.0), axis=0, keepdims=True)

    id_rows = lanes(ids[...], -1.0)
    wt_rows = lanes(wts[...], 0.0)
    earlier = lane < at
    facts = []
    for k in range(2):
        col = column(id_rows[k : k + 1])
        same = jnp.where(id_rows[0:1] == col, 1.0, 0.0) + jnp.where(id_rows[1:2] == col, 1.0, 0.0)
        rank = jnp.sum(jnp.where(earlier, same, 0.0), axis=1, keepdims=True)
        facts.append(moved(col * 4.0 + rank))
    for k in range(2):
        facts.append(moved(column(wt_rows[k : k + 1])))
    facts.append(jnp.zeros((4, 128), F32))
    rt[z] = jnp.concatenate(facts, axis=0)

    pl.semaphore_wait(barrier, 19)

    def rt_copy(k):
        return remote(rt.at[z], rt.at[z], rts.at[k], rtr.at[k], ep=z_ep(k))

    for k in NEAR:
        rt_copy(k).start()

    def w_copy(i):
        block = (z + 4 + (0, 0, 0, 0, -1, 1, -1, 1)[i]) % 4
        ref = (
            wdg.at[:, block], wdg.at[:, block], ddg.at[:, block], ddg.at[:, block],
            wdg.at[0, block], wdg.at[1, block], ddg.at[0, block], ddg.at[1, block],
        )[i]
        return remote(ref, ref, wss.at[i], wrs.at[i], ep=z_ep((1, -1)[i % 2]))

    def w_wait(i):
        block = (z + 4 + (-1, 1, -1, 1, -2, 2, -2, 2)[i]) % 4
        ref = (
            wdg.at[:, block], wdg.at[:, block], ddg.at[:, block], ddg.at[:, block],
            wdg.at[0, block], wdg.at[1, block], ddg.at[0, block], ddg.at[1, block],
        )[i]
        remote(ref, ref, wss.at[i], wrs.at[i], tp=other).wait_recv()

    for i in (2, 3, 0, 1):
        w_copy(i).start()

    h = hid[...].astype(F32)
    normed = (h * lax.rsqrt(jnp.mean(h * h, axis=-1, keepdims=True) + EPS) * again[...]).astype(BF)
    angles = column(lanes(prow[...], 0.0)) * freq[...]
    cos = jnp.cos(angles)
    low = (lane & 63) < 32
    sin = jnp.sin(angles) * jnp.where(low, -1.0, 1.0)

    def rotated(v):
        turned = jnp.where(low, pltpu.roll(v, 96, 1), pltpu.roll(v, 32, 1))
        return (v * cos + turned * sin).astype(BF)

    for cp in first:
        cp.wait()
    new_k = rotated(dot(normed, wk[...]))
    new_v = dot(normed, wv[...]).astype(BF)
    out[:, HALF : HALF + 128] = new_k
    out[:, HALF + 128 : HALF + 256] = new_v
    kn[...] = new_k.astype(F32)
    vn[...] = new_v.astype(F32)
    q = dot(normed, wq[...])
    for i in range(8):
        qs[:, i, :] = rotated(q[:, i * 128 : (i + 1) * 128]).astype(F32) * 0.125

    lam_col = jnp.zeros((8, 128), F32)
    rows8 = lax.broadcasted_iota(jnp.int32, (8, 128), 0)
    for i in range(8):
        lam_col = jnp.where(rows8 == i, lam[i], lam_col)
    left = lax.broadcasted_iota(jnp.int32, (8, 128), 1) < 64
    last16 = lax.broadcasted_iota(jnp.int32, (16, 128), 0) == 15
    places = lax.broadcasted_iota(jnp.int32, (16, CACHE), 1)
    gain = hgain[...]

    @pl.loop(0, NGRP)
    def _(g):
        for cp in kv(g):
            cp.wait()

        @pl.when(g + AHEAD < NGRP)
        def _():
            for cp in kv(g + AHEAD):
                cp.start()

        @pl.when(g + AHEAD == NGRP)
        def _():
            later[0].start()

        sums, parts = [], []
        for i in range(GRP):
            s = g * GRP + i
            tail = pl.ds(CACHE - 16, 16)
            kb[s, tail, :] = jnp.where(
                last16, jnp.broadcast_to(kn[pl.ds(s, 1), :], (16, 128)), kb[s, tail, :].astype(F32)
            ).astype(BF)
            vb[s, tail, :] = jnp.where(
                last16, jnp.broadcast_to(vn[pl.ds(s, 1), :], (16, 128)), vb[s, tail, :].astype(F32)
            ).astype(BF)
            qv = qs[s]
            q2 = jnp.concatenate(
                [jnp.where(left, qv, 0.0), jnp.where(left, 0.0, qv)], axis=0
            ).astype(BF)
            scores = dot_nt(q2, kb[s])
            usable = (places < plen[s]) | (places == CACHE - 1)
            scores = jnp.where(usable, scores, -jnp.inf)
            peak = jnp.max(scores, axis=-1, keepdims=True)
            weights = jnp.exp(scores - peak)
            sums.append(jnp.sum(weights, axis=-1, keepdims=True))
            parts.append(weights.astype(BF))
        for i in range(0, GRP, 2):
            s = g * GRP + i
            values = jnp.concatenate([vb[s], vb[s + 1]], axis=1)
            pair = dot(jnp.concatenate(parts[i : i + 2], axis=0), values)
            for j in range(2):
                mapped = pair[16 * j : 16 * j + 16, 128 * j : 128 * j + 128] / sums[i + j]
                mix = mapped[0:8] - lam_col * mapped[8:16]
                ho[s + j] = mix * lax.rsqrt(jnp.mean(mix * mix, axis=-1, keepdims=True) + EPS) * gain

    for cp in later[1:]:
        cp.start()
    later[0].wait()
    head_out = jnp.concatenate([ho[:, i, :].astype(BF) for i in range(8)], axis=1)
    pbuf[0] = dot(head_out, wo[...]).astype(BF)
    tp_copy = remote(pbuf.at[0], pbuf.at[1], tps, tpr, tp=other)
    tp_copy.start()
    for i in (2, 3, 0, 1):
        w_wait(i)
        w_copy(4 + i).start()
    tp_copy.wait()
    attn_out = (pbuf[0].astype(F32) + pbuf[1].astype(F32)).astype(BF)
    res = hid[...].astype(F32) + attn_out.astype(F32)
    resid[...] = res
    G[b * 4 + a] = (
        res * lax.rsqrt(jnp.mean(res * res, axis=-1, keepdims=True) + EPS) * fgain[...]
    ).astype(BF)

    def g_copy(ka, kb_, da, db):
        src = ((b + 4 - kb_) % 4) * 4 + (a + 4 - ka) % 4
        dest = zb + pidx((a + da) % 4, (b + db) % 4)
        i = (ka + da) * 4 + kb_ + db
        ref = G.at[src, :, half]
        return remote(ref, ref, gss.at[i], grs.at[i], ep=dest)

    def g_share(ka, kb_):
        aa, bb = (a + 4 - ka) % 4, (b + 4 - kb_) % 4
        i = kb_ * 4 + ka
        return remote(
            G.at[bb * 4 + aa, :, half], G.at[aa * 4 + bb, :, half], gds.at[i], gdr.at[i], tp=other
        )

    def g_arrive(ka, kb_):
        i = ka * 4 + kb_
        ref = G.at[((b + 4 - kb_) % 4) * 4 + (a + 4 - ka) % 4, :, half]
        remote(ref, ref, gss.at[i], grs.at[i], tp=other).wait_recv()
        g_share(ka, kb_).start()

    own_block = G.at[b * 4 + a, :, half]

    def zg_copy(k):
        return remote(own_block, zg.at[z], zs.at[k], zr.at[k], ep=z_ep(k))

    for k in NEAR:
        zg_copy(k).start()
        g_copy(0, 0, k, 0).start()
        g_copy(0, 0, 0, k).start()
    zg[z] = G[b * 4 + a, :, half]

    for k in NEAR:
        ref = rt.at[(z + 4 - k) % 4]
        remote(ref, ref, rts.at[k], rtr.at[k], tp=other).wait_recv()
    facts = rt[0] + rt[1] + rt[2] + rt[3]
    row = lax.broadcasted_iota(jnp.int32, (256, 128), 0)
    token = lax.broadcasted_iota(jnp.int32, (256, 128), 1)
    target = (((zb + (row >> 4)) >> 1) * 4 + (row & 3)).astype(F32)
    mine = ((row >> 2) & 3) == (token >> 5)
    hit0 = mine & (facts[0:1] == target)
    hit1 = mine & (facts[1:2] == target)
    sel[...] = jnp.where(hit0 | hit1, 1.0, 0.0).astype(BF)
    selw[...] = (jnp.where(hit0, facts[2:3], 0.0) + jnp.where(hit1, facts[3:4], 0.0)).astype(BF)

    for ka in NEAR:
        g_arrive(ka, 0)
    for k in NEAR:
        for ka in NEAR:
            g_copy(ka, 0, 0, k).start()

    def mate(dy, dx):
        return ((y + 4 + dy) % 4) * 4 + (x + 4 + dx) % 4

    def x_copy(dy, dx):
        i = dy * 4 + dx
        to = mate(dy, dx)
        return remote(D.at[to], X.at[p0], xs.at[i], xr.at[i], ep=zb + to)

    def y_copy(dy, dx):
        i = dy * 4 + dx
        to = mate(dy, dx)
        return remote(Y.at[to], R.at[p0], ys.at[i], yr.at[i], ep=zb + to)

    for k in NEAR:
        ref = zg.at[(z + 4 - k) % 4]
        remote(ref, ref, zs.at[k], zr.at[k], tp=other).wait_recv()
    D[...] = dot(sel[...], zg[...].reshape(128, HALF)).astype(BF).reshape(16, 16, HALF)
    for dy, dx in MATES:
        x_copy(dy, dx).start()
    X[p0] = D[p0]

    for k in NEAR:
        for ka in (0, 1, 3, 2):
            g_arrive(ka, k)
    for i in range(4, 8):
        w_wait(i)
    for ka in range(4):
        for kb_ in range(4):
            if ka or kb_:
                i = ka * 4 + kb_
                ref = G.at[((b + 4 - kb_) % 4) * 4 + (a + 4 - ka) % 4, :, other_half]
                remote(ref, ref, gds.at[i], gdr.at[i], tp=other).wait_recv()

    @pl.loop(0, 4)
    def _(g):
        tokens = G[pl.ds(g * 4, 4)].reshape(128, WIDTH)
        pre_gate = dot_nt(tokens, wdg[0].reshape(192, WIDTH))
        pre_up = dot_nt(tokens, wdg[1].reshape(192, WIDTH))
        act = pre_gate / (1.0 + jnp.exp(-pre_gate)) * pre_up
        act = jnp.concatenate([act, jnp.zeros((128, 64), F32)], axis=1).astype(BF)
        dact[0, pl.ds(g * 4, 4)] = act.reshape(4, ROWS, 256)
        mix_gate = (1.0 / (1.0 + jnp.exp(-pre_gate[:, 44:45]))).astype(BF).astype(F32)
        gsc[g] = jnp.broadcast_to(mix_gate, (128, 128))

    act_copy = remote(dact.at[0], dact.at[1], das, dar, tp=other)
    act_copy.start()

    def x_share(dy):
        rows = pl.ds(((y + 4 - dy) % 4) * 4, 4)
        return remote(X.at[rows], Xo.at[rows], xds.at[dy], xdr.at[dy], tp=other)

    for dy in (0, 1, 3, 2):
        for dx in range(4):
            if dy or dx:
                i = dy * 4 + dx
                ref = X.at[mate(-dy, -dx)]
                remote(ref, ref, xs.at[i], xr.at[i], tp=other).wait_recv()
        x_share(dy).start()

    def r1_copy(k):
        to = (b + k) % 4
        return remote(pb.at[to], s1.at[k - 1], r1s.at[k], r1r.at[k], ep=zb + pidx(a, to))

    def r2_copy(k):
        to = (a + k) % 4
        return remote(tb.at[to], s2.at[k - 1], r2s.at[k], r2r.at[k], ep=zb + pidx(to, b))

    remote(dact.at[0], dact.at[1], das, dar, tp=other).wait_recv()
    for kb_ in (1, 3, 2, 0):
        g = (b + kb_) % 4
        other_act = jnp.concatenate([dact[1, i * 4 + g] for i in range(4)], axis=0)
        part = dot(dact[0, pl.ds(g * 4, 4)].reshape(128, 256)[:, :192], ddg[c].reshape(192, HALF)) + dot(
            other_act[:, :192], ddg[other].reshape(192, HALF)
        )
        pb[g] = (part * gsc[g][:, 0:1]).astype(BF).reshape(4, ROWS, HALF)
        if kb_:
            r1_copy(kb_).start()

    for cp in later[1:]:
        cp.wait()
    for dy in (0, 1, 3, 2):
        rows = pl.ds(((y + 4 - dy) % 4) * 4, 4)
        remote(X.at[rows], Xo.at[rows], xds.at[dy], xdr.at[dy], tp=other).wait_recv()
    own_rows = X[...].reshape(256, HALF)
    other_rows = Xo[...].reshape(256, HALF)
    gate_pre = dot_nt(own_rows, eg[:, half]) + dot_nt(other_rows, eg[:, other_half])
    up_pre = dot_nt(own_rows, eu[:, half]) + dot_nt(other_rows, eu[:, other_half])
    inner = gate_pre / (1.0 + jnp.exp(-gate_pre)) * up_pre
    abuf[0] = jnp.concatenate([inner, jnp.zeros((256, 32), F32)], axis=1).astype(BF)
    a_copy = remote(abuf.at[0], abuf.at[1], as_, ar, tp=other)
    a_copy.start()
    own_ed = ed[pl.ds(pl.multiple_of(c * 352, 32), 352), :]
    other_ed = ed[pl.ds(pl.multiple_of(other * 352, 32), 352), :]
    down = dot(abuf[0][:, :352], own_ed)
    remote(abuf.at[0], abuf.at[1], as_, ar, tp=other).wait_recv()
    down = down + dot(abuf[1][:, :352], other_ed)
    Y[...] = down.astype(BF).reshape(16, 16, HALF)

    for dy, dx in MATES:
        y_copy(dy, dx).start()
    R[p0] = Y[p0]
    for k in NEAR:
        r1_copy(k).wait_recv()
    tb[...] = (
        pb[b].astype(F32) + s1[0].astype(F32) + s1[1].astype(F32) + s1[2].astype(F32)
    ).astype(BF)
    for k in NEAR:
        r2_copy(k).start()
    for dy, dx in MATES:
        i = dy * 4 + dx
        ref = R.at[mate(-dy, -dx)]
        remote(ref, ref, ys.at[i], yr.at[i], tp=other).wait_recv()
    M[...] = dot_tn(selw[...], R[...].reshape(256, HALF)).astype(BF).reshape(4, ROWS, HALF)

    def m_copy(k):
        return remote(M.at[(z + k) % 4], m_in.at[k - 1], ms.at[k], mr.at[k], ep=z_ep(k))

    for k in NEAR:
        m_copy(k).start()
    for k in NEAR:
        r2_copy(k).wait_recv()
    final = tb[a].astype(F32) + s2[0].astype(F32) + s2[1].astype(F32) + s2[2].astype(F32)
    final = resid[:, half] + final + M[z].astype(F32)
    for k in NEAR:
        m_copy(k).wait_recv()
    final = final + m_in[0].astype(F32) + m_in[1].astype(F32) + m_in[2].astype(F32)
    out[:, :HALF] = final.astype(BF)

    for i in range(8):
        w_copy(i).wait_send()
    for k in NEAR:
        rt_copy(k).wait_send()
        zg_copy(k).wait_send()
        m_copy(k).wait_send()
        g_copy(0, 0, k, 0).wait_send()
        g_copy(0, 0, 0, k).wait_send()
        r1_copy(k).wait_send()
        r2_copy(k).wait_send()
        for i in NEAR:
            g_copy(i, 0, 0, k).wait_send()
    for dy, dx in MATES:
        x_copy(dy, dx).wait_send()
        y_copy(dy, dx).wait_send()
        g_share(dy, dx).wait_send()
    for k in range(4):
        x_share(k).wait_send()
    act_copy.wait_send()
    a_copy.wait_send()


def split_kernel(both, out, nk, nv, sem):
    copies = [
        pltpu.make_async_copy(both.at[:, pl.ds(0, HALF)], out, sem.at[0]),
        pltpu.make_async_copy(both.at[:, pl.ds(HALF, 128)], nk, sem.at[1]),
        pltpu.make_async_copy(both.at[:, pl.ds(HALF + 128, 128)], nv, sem.at[2]),
    ]
    for cp in copies:
        cp.start()
    for cp in copies:
        cp.wait()


def per_device(
    hidden_in, past_lengths, key_cache, value_cache, attn_gain, w_query, w_key, w_value,
    lambdas, head_gain, w_out, ffn_gain, route_ids, route_weights, expert_gate, expert_up,
    expert_down, gate_vector, dense_gate, dense_up, dense_down,
):
    freq = np.power(np.float32(ROPE_BASE), -(np.arange(128) % 32).astype(np.float32) / np.float32(32))
    freq = jnp.asarray(freq.astype(np.float32)[None])
    vm = pl.BlockSpec(memory_space=pltpu.VMEM)
    sm = pl.BlockSpec(memory_space=pltpu.SMEM)
    hbm = pl.BlockSpec(memory_space=pl.ANY)
    V = pltpu.VMEM
    dma = pltpu.SemaphoreType.DMA
    scratch = [
        V((ROWS, CACHE, 128), BF), V((ROWS, CACHE, 128), BF),
        V((WIDTH, 1024), BF), V((WIDTH, 128), BF), V((WIDTH, 128), BF), V((1024, WIDTH), BF),
        V((352, WIDTH), BF), V((352, WIDTH), BF), V((704, HALF), BF),
        V((44, WIDTH), BF), V((44, WIDTH), BF), V((48, HALF), BF),
        V((2, 4, 48, WIDTH), BF), V((2, 4, 48, HALF), BF),
        V((ROWS, 8, 128), F32), V((ROWS, 128), F32), V((ROWS, 128), F32), V((ROWS, 8, 128), F32),
        V((2, ROWS, WIDTH), BF), V((ROWS, WIDTH), F32), V((4, 8, 128), F32),
        V((16, ROWS, WIDTH), BF), V((4, ROWS, HALF), BF), V((16, 16, HALF), BF),
        V((16, 16, HALF), BF), V((16, 16, HALF), BF), V((2, 256, 384), BF), V((16, 16, HALF), BF),
        V((16, 16, HALF), BF), V((4, ROWS, HALF), BF), V((3, ROWS, HALF), BF),
        V((2, 16, ROWS, 256), BF), V((4, 128, 128), F32), V((256, 128), BF), V((256, 128), BF),
        V((4, 4, ROWS, HALF), BF), V((3, 4, ROWS, HALF), BF), V((4, ROWS, HALF), BF),
        V((3, ROWS, HALF), BF),
        dma((11,)), dma((2, NGRP)), dma((8,)), dma((8,)), dma, dma,
        dma((4,)), dma((4,)),
        dma((16,)), dma((16,)), dma((16,)), dma((16,)), dma((4,)), dma((4,)), dma((16,)), dma((16,)),
        dma((4,)), dma((4,)), dma, dma, dma, dma, dma((16,)), dma((16,)),
        dma((4,)), dma((4,)), dma((4,)), dma((4,)), dma((4,)), dma((4,)),
    ]
    both = pl.pallas_call(
        layer_kernel,
        name="layer",
        out_shape=jax.ShapeDtypeStruct((ROWS, HALF + 256), BF),
        in_specs=[vm, vm, sm, vm, vm, sm, vm, vm, vm, vm, vm] + [hbm] * 12,
        out_specs=vm,
        scratch_shapes=scratch,
        compiler_params=pltpu.CompilerParams(
            collective_id=0, has_side_effects=True, vmem_limit_bytes=VMEM_BYTES
        ),
    )(
        hidden_in, freq, past_lengths, past_lengths.reshape(1, ROWS), attn_gain.reshape(1, WIDTH),
        lambdas, head_gain.reshape(1, 128), ffn_gain.reshape(1, WIDTH), route_ids.T,
        route_weights.T, gate_vector.reshape(16, 128),
        key_cache, value_cache, w_query, w_key, w_value, w_out,
        expert_gate.swapaxes(1, 2), expert_up.swapaxes(1, 2), expert_down,
        dense_gate.T, dense_up.T, dense_down,
    )
    return pl.pallas_call(
        split_kernel,
        name="split",
        out_shape=(
            jax.ShapeDtypeStruct((ROWS, HALF), BF),
            jax.ShapeDtypeStruct((ROWS, 128), BF),
            jax.ShapeDtypeStruct((ROWS, 128), BF),
        ),
        in_specs=[hbm],
        out_specs=(hbm, hbm, hbm),
        scratch_shapes=[dma((3,))],
        compiler_params=pltpu.CompilerParams(vmem_limit_bytes=1 << 20),
    )(both)


def solution(mesh):
    return jax.shard_map(
        per_device,
        mesh=mesh,
        in_specs=(
            P("ep", None), P("ep"), P("ep", None, "tp"), P("ep", None, "tp"), P(),
            P(None, "tp"), P(None, "tp"), P(None, "tp"), P("tp"), P(), P("tp", None), P(),
            P("ep", None), P("ep", None), P("ep", None, "tp"), P("ep", None, "tp"),
            P("ep", None, "tp"), P(), P(None, ("ep", "tp")), P(None, ("ep", "tp")), P("ep", "tp"),
        ),
        out_specs=(P("ep", "tp"), P("ep", "tp"), P("ep", "tp")),
        check_vma=False,
    )
```

```python
import jax
import jax.numpy as jnp
import numpy as np
from jax import lax
from jax.experimental import pallas as pl
from jax.experimental.pallas import tpu as pltpu
from jax.sharding import PartitionSpec as P

EPS = 1e-05
ROPE_BASE = 10000.0
BF = jnp.bfloat16
F32 = jnp.float32
ROWS = 32
WIDTH = 2048
HALF = 1024
CACHE = 1024
GRP = 8
NGRP = ROWS // GRP
AHEAD = 2
VMEM_BYTES = 66 * 1000 * 1000
NEAR = (1, 3, 2)
MATES = tuple((i // 4, i % 4) for i in (10, 6, 14, 9, 11, 2, 8, 5, 7, 13, 15, 1, 3, 4, 12))
NT = (((1,), (1,)), ((), ()))
TN = (((0,), (0,)), ((), ()))


def dot(a, b):
    return jnp.dot(a, b, preferred_element_type=F32)


def dot_nt(a, b):
    return lax.dot_general(a, b, NT, preferred_element_type=F32)


def dot_tn(a, b):
    return lax.dot_general(a, b, TN, preferred_element_type=F32)


def layer_kernel(
    hid, freq, plen, prow, again, lam, hgain, fgain, ids, wts, gvec,
    kc_h, vc_h, wq_h, wk_h, wv_h, wo_h, eg_h, eu_h, ed_h, dg_h, du_h, dd_h,
    out,
    kb, vb, wq, wk, wv, wo, eg, eu, ed, dg, du, dtail,
    wdg, ddg, qs, kn, vn, ho, pbuf, resid, rt, G, zg, D, X, Xo, abuf, Y, R, M, m_in,
    dact, gsc, sel, selw, pb, s1, tb, s2,
    lsem, kvsem, wss, wrs, tps, tpr, rts, rtr,
    gss, grs, gds, gdr, zs, zr, xs, xr, xds, xdr, as_, ar, das, dar, ys, yr,
    r1s, r1r, r2s, r2r, ms, mr,
):
    c = lax.axis_index("tp")
    ep = lax.axis_index("ep")
    z = ep // 16
    p0 = ep % 16
    y = p0 // 4
    x = p0 % 4
    sa = 1 + 3 * c
    sb = 4 - 3 * c
    a = x * (1 - c) + y * c
    b = y * (1 - c) + x * c
    zb = z * 16
    other = 1 - c
    half = pl.ds(pl.multiple_of(c * HALF, HALF), HALF)
    other_half = pl.ds(pl.multiple_of(other * HALF, HALF), HALF)

    def local(src, dst, sem):
        return pltpu.make_async_copy(src, dst, sem)

    def remote(src, dst, ssem, rsem, **dev):
        return pltpu.make_async_remote_copy(
            src_ref=src, dst_ref=dst, send_sem=ssem, recv_sem=rsem,
            device_id=dev, device_id_type=pl.DeviceIdType.MESH,
        )

    def pidx(aa, bb):
        return aa * sa + bb * sb

    def z_ep(step):
        return ((z + 4 + step) % 4) * 16 + p0

    own_w = [
        local(dg_h, dg, lsem.at[3]),
        local(du_h, du, lsem.at[4]),
        local(dd_h.at[pl.ds(0, 48)], ddg.at[0, z], lsem.at[9]),
        local(dd_h.at[pl.ds(40, 48)], dtail, lsem.at[10]),
    ]
    first = [
        local(wk_h, wk, lsem.at[1]),
        local(wv_h, wv, lsem.at[2]),
        local(wq_h, wq, lsem.at[0]),
    ]
    for cp in own_w + first:
        cp.start()

    def kv(g):
        rows = pl.ds(g * GRP, GRP)
        return (
            local(kc_h.at[rows], kb.at[rows], kvsem.at[0, g]),
            local(vc_h.at[rows], vb.at[rows], kvsem.at[1, g]),
        )

    later = [
        local(wo_h, wo, lsem.at[5]),
        local(eg_h.at[0], eg, lsem.at[6]),
        local(eu_h.at[0], eu, lsem.at[7]),
        local(ed_h.at[0], ed, lsem.at[8]),
    ]

    barrier = pltpu.get_barrier_semaphore()
    for k in range(1, 16):
        dest = zb + ((y + k // 4) % 4) * 4 + (x + k % 4) % 4
        pl.semaphore_signal(barrier, inc=1, device_id={"ep": dest}, device_id_type=pl.DeviceIdType.MESH)
    for step in NEAR:
        pl.semaphore_signal(barrier, inc=1, device_id={"ep": z_ep(step)}, device_id_type=pl.DeviceIdType.MESH)
    pl.semaphore_signal(barrier, inc=1, device_id={"tp": other}, device_id_type=pl.DeviceIdType.MESH)

    for cp in own_w:
        cp.wait()
    gv = gvec[...].astype(F32)
    gv = jnp.concatenate([gv[i : i + 1] for i in range(16)], axis=1)
    pad_row = lax.broadcasted_iota(jnp.int32, (4, WIDTH), 0)
    wdg[0, z, 0:44, :] = dg[...]
    wdg[0, z, 44:48, :] = jnp.where(pad_row == 0, gv, 0.0).astype(BF)
    wdg[1, z, 0:44, :] = du[...]
    wdg[1, z, 44:48, :] = jnp.zeros((4, WIDTH), BF)
    ddg[1, z] = pltpu.roll(dtail[...].astype(F32), 44, 0).astype(BF)

    at = lax.broadcasted_iota(jnp.int32, (ROWS, 128), 0)
    lane = lax.broadcasted_iota(jnp.int32, (ROWS, 128), 1)
    diag = at == lane
    shifted = at + 32 * z == lane

    def lanes(v, fill):
        return jnp.concatenate([v.astype(F32), jnp.full((v.shape[0], 128 - ROWS), fill, F32)], axis=1)

    def column(v):
        return jnp.sum(jnp.where(diag, v, 0.0), axis=1, keepdims=True)

    def moved(col):
        return jnp.sum(jnp.where(shifted, col, 0.0), axis=0, keepdims=True)

    id_rows = lanes(ids[...], -1.0)
    wt_rows = lanes(wts[...], 0.0)
    earlier = lane < at
    facts = []
    for k in range(2):
        col = column(id_rows[k : k + 1])
        same = jnp.where(id_rows[0:1] == col, 1.0, 0.0) + jnp.where(id_rows[1:2] == col, 1.0, 0.0)
        rank = jnp.sum(jnp.where(earlier, same, 0.0), axis=1, keepdims=True)
        facts.append(moved(col * 4.0 + rank))
    for k in range(2):
        facts.append(moved(column(wt_rows[k : k + 1])))
    facts.append(jnp.zeros((4, 128), F32))
    rt[z] = jnp.concatenate(facts, axis=0)

    for g in range(AHEAD):
        for cp in kv(g):
            cp.start()

    pl.semaphore_wait(barrier, 19)

    def rt_copy(k):
        return remote(rt.at[z], rt.at[z], rts.at[k], rtr.at[k], ep=z_ep(k))

    for k in NEAR:
        rt_copy(k).start()

    def w_copy(i):
        block = (z + 4 + (0, 0, 0, 0, -1, 1, -1, 1)[i]) % 4
        ref = (
            wdg.at[:, block], wdg.at[:, block], ddg.at[:, block], ddg.at[:, block],
            wdg.at[0, block], wdg.at[1, block], ddg.at[0, block], ddg.at[1, block],
        )[i]
        return remote(ref, ref, wss.at[i], wrs.at[i], ep=z_ep((1, -1)[i % 2]))

    def w_wait(i):
        block = (z + 4 + (-1, 1, -1, 1, -2, 2, -2, 2)[i]) % 4
        ref = (
            wdg.at[:, block], wdg.at[:, block], ddg.at[:, block], ddg.at[:, block],
            wdg.at[0, block], wdg.at[1, block], ddg.at[0, block], ddg.at[1, block],
        )[i]
        remote(ref, ref, wss.at[i], wrs.at[i], tp=other).wait_recv()

    for i in (2, 3, 0, 1):
        w_copy(i).start()

    h = hid[...].astype(F32)
    normed = (h * lax.rsqrt(jnp.mean(h * h, axis=-1, keepdims=True) + EPS) * again[...]).astype(BF)
    angles = column(lanes(prow[...], 0.0)) * freq[...]
    cos = jnp.cos(angles)
    low = (lane & 63) < 32
    sin = jnp.sin(angles) * jnp.where(low, -1.0, 1.0)

    def rotated(v):
        turned = jnp.where(low, pltpu.roll(v, 96, 1), pltpu.roll(v, 32, 1))
        return (v * cos + turned * sin).astype(BF)

    for cp in first:
        cp.wait()
    new_k = rotated(dot(normed, wk[...]))
    new_v = dot(normed, wv[...]).astype(BF)
    out[:, HALF : HALF + 128] = new_k
    out[:, HALF + 128 : HALF + 256] = new_v
    kn[...] = new_k.astype(F32)
    vn[...] = new_v.astype(F32)
    q = dot(normed, wq[...])
    for i in range(8):
        qs[:, i, :] = rotated(q[:, i * 128 : (i + 1) * 128]).astype(F32) * 0.125

    lam_col = jnp.zeros((8, 128), F32)
    rows8 = lax.broadcasted_iota(jnp.int32, (8, 128), 0)
    for i in range(8):
        lam_col = jnp.where(rows8 == i, lam[i], lam_col)
    left = lax.broadcasted_iota(jnp.int32, (8, 128), 1) < 64
    last16 = lax.broadcasted_iota(jnp.int32, (16, 128), 0) == 15
    places = lax.broadcasted_iota(jnp.int32, (16, CACHE), 1)
    gain = hgain[...]

    @pl.loop(0, NGRP)
    def _(g):
        for cp in kv(g):
            cp.wait()

        @pl.when(g + AHEAD < NGRP)
        def _():
            for cp in kv(g + AHEAD):
                cp.start()

        @pl.when(g + AHEAD == NGRP)
        def _():
            later[0].start()

        sums, parts = [], []
        for i in range(GRP):
            s = g * GRP + i
            tail = pl.ds(CACHE - 16, 16)
            kb[s, tail, :] = jnp.where(
                last16, jnp.broadcast_to(kn[pl.ds(s, 1), :], (16, 128)), kb[s, tail, :].astype(F32)
            ).astype(BF)
            vb[s, tail, :] = jnp.where(
                last16, jnp.broadcast_to(vn[pl.ds(s, 1), :], (16, 128)), vb[s, tail, :].astype(F32)
            ).astype(BF)
            qv = qs[s]
            q2 = jnp.concatenate(
                [jnp.where(left, qv, 0.0), jnp.where(left, 0.0, qv)], axis=0
            ).astype(BF)
            scores = dot_nt(q2, kb[s])
            usable = (places < plen[s]) | (places == CACHE - 1)
            scores = jnp.where(usable, scores, -jnp.inf)
            peak = jnp.max(scores, axis=-1, keepdims=True)
            weights = jnp.exp(scores - peak)
            sums.append(jnp.sum(weights, axis=-1, keepdims=True))
            parts.append(weights.astype(BF))
        for i in range(0, GRP, 2):
            s = g * GRP + i
            values = jnp.concatenate([vb[s], vb[s + 1]], axis=1)
            pair = dot(jnp.concatenate(parts[i : i + 2], axis=0), values)
            for j in range(2):
                mapped = pair[16 * j : 16 * j + 16, 128 * j : 128 * j + 128] / sums[i + j]
                mix = mapped[0:8] - lam_col * mapped[8:16]
                ho[s + j] = mix * lax.rsqrt(jnp.mean(mix * mix, axis=-1, keepdims=True) + EPS) * gain

    for cp in later[1:]:
        cp.start()
    later[0].wait()
    head_out = jnp.concatenate([ho[:, i, :].astype(BF) for i in range(8)], axis=1)
    pbuf[0] = dot(head_out, wo[...]).astype(BF)
    tp_copy = remote(pbuf.at[0], pbuf.at[1], tps, tpr, tp=other)
    tp_copy.start()
    tp_copy.wait()
    attn_out = (pbuf[0].astype(F32) + pbuf[1].astype(F32)).astype(BF)
    res = hid[...].astype(F32) + attn_out.astype(F32)
    resid[...] = res
    G[b * 4 + a] = (
        res * lax.rsqrt(jnp.mean(res * res, axis=-1, keepdims=True) + EPS) * fgain[...]
    ).astype(BF)

    def g_copy(ka, kb_, da, db):
        src = ((b + 4 - kb_) % 4) * 4 + (a + 4 - ka) % 4
        dest = zb + pidx((a + da) % 4, (b + db) % 4)
        i = (ka + da) * 4 + kb_ + db
        ref = G.at[src, :, half]
        return remote(ref, ref, gss.at[i], grs.at[i], ep=dest)

    def g_share(ka, kb_):
        aa, bb = (a + 4 - ka) % 4, (b + 4 - kb_) % 4
        i = kb_ * 4 + ka
        return remote(
            G.at[bb * 4 + aa, :, half], G.at[aa * 4 + bb, :, half], gds.at[i], gdr.at[i], tp=other
        )

    def g_arrive(ka, kb_):
        i = ka * 4 + kb_
        ref = G.at[((b + 4 - kb_) % 4) * 4 + (a + 4 - ka) % 4, :, half]
        remote(ref, ref, gss.at[i], grs.at[i], tp=other).wait_recv()
        g_share(ka, kb_).start()

    own_block = G.at[b * 4 + a, :, half]

    def zg_copy(k):
        return remote(own_block, zg.at[z], zs.at[k], zr.at[k], ep=z_ep(k))

    for k in NEAR:
        g_copy(0, 0, k, 0).start()
        zg_copy(k).start()
    zg[z] = G[b * 4 + a, :, half]

    for k in NEAR:
        ref = rt.at[(z + 4 - k) % 4]
        remote(ref, ref, rts.at[k], rtr.at[k], tp=other).wait_recv()
    facts = rt[0] + rt[1] + rt[2] + rt[3]
    row = lax.broadcasted_iota(jnp.int32, (256, 128), 0)
    token = lax.broadcasted_iota(jnp.int32, (256, 128), 1)
    target = (((zb + (row >> 4)) >> 1) * 4 + (row & 3)).astype(F32)
    mine = ((row >> 2) & 3) == (token >> 5)
    hit0 = mine & (facts[0:1] == target)
    hit1 = mine & (facts[1:2] == target)
    sel[...] = jnp.where(hit0 | hit1, 1.0, 0.0).astype(BF)
    selw[...] = (jnp.where(hit0, facts[2:3], 0.0) + jnp.where(hit1, facts[3:4], 0.0)).astype(BF)

    for i in (2, 3):
        w_wait(i)
        w_copy(4 + i).start()

    for ka in NEAR:
        g_arrive(ka, 0)
        if ka == 1:
            for k in NEAR:
                g_copy(0, 0, 0, k).start()
    for k in NEAR:
        for ka in NEAR:
            g_copy(ka, 0, 0, k).start()

    def mate(dy, dx):
        return ((y + 4 + dy) % 4) * 4 + (x + 4 + dx) % 4

    def x_copy(dy, dx):
        i = dy * 4 + dx
        to = mate(dy, dx)
        return remote(D.at[to], X.at[p0], xs.at[i], xr.at[i], ep=zb + to)

    def y_copy(dy, dx):
        i = dy * 4 + dx
        to = mate(dy, dx)
        return remote(Y.at[to], R.at[p0], ys.at[i], yr.at[i], ep=zb + to)

    for k in NEAR:
        ref = zg.at[(z + 4 - k) % 4]
        remote(ref, ref, zs.at[k], zr.at[k], tp=other).wait_recv()
    D[...] = dot(sel[...], zg[...].reshape(128, HALF)).astype(BF).reshape(16, 16, HALF)
    for dy, dx in MATES:
        x_copy(dy, dx).start()
    for i in (0, 1):
        w_wait(i)
        w_copy(4 + i).start()
    X[p0] = D[p0]

    for k in NEAR:
        for ka in (0, 1, 3, 2):
            g_arrive(ka, k)
    for i in range(4, 8):
        w_wait(i)
    for ka in range(4):
        for kb_ in range(4):
            if ka or kb_:
                i = ka * 4 + kb_
                ref = G.at[((b + 4 - kb_) % 4) * 4 + (a + 4 - ka) % 4, :, other_half]
                remote(ref, ref, gds.at[i], gdr.at[i], tp=other).wait_recv()

    @pl.loop(0, 4)
    def _(g):
        tokens = G[pl.ds(g * 4, 4)].reshape(128, WIDTH)
        pre_gate = dot_nt(tokens, wdg[0].reshape(192, WIDTH))
        pre_up = dot_nt(tokens, wdg[1].reshape(192, WIDTH))
        act = pre_gate / (1.0 + jnp.exp(-pre_gate)) * pre_up
        act = jnp.concatenate([act, jnp.zeros((128, 64), F32)], axis=1).astype(BF)
        dact[0, pl.ds(g * 4, 4)] = act.reshape(4, ROWS, 256)
        mix_gate = (1.0 / (1.0 + jnp.exp(-pre_gate[:, 44:45]))).astype(BF).astype(F32)
        gsc[g] = jnp.broadcast_to(mix_gate, (128, 128))

    act_copy = remote(dact.at[0], dact.at[1], das, dar, tp=other)
    act_copy.start()

    def x_share(dy):
        rows = pl.ds(((y + 4 - dy) % 4) * 4, 4)
        return remote(X.at[rows], Xo.at[rows], xds.at[dy], xdr.at[dy], tp=other)

    for dy in (0, 1, 3, 2):
        for dx in range(4):
            if dy or dx:
                i = dy * 4 + dx
                ref = X.at[mate(-dy, -dx)]
                remote(ref, ref, xs.at[i], xr.at[i], tp=other).wait_recv()
        x_share(dy).start()

    def r1_copy(k):
        to = (b + k) % 4
        return remote(pb.at[to], s1.at[k - 1], r1s.at[k], r1r.at[k], ep=zb + pidx(a, to))

    def r2_copy(k):
        to = (a + k) % 4
        return remote(tb.at[to], s2.at[k - 1], r2s.at[k], r2r.at[k], ep=zb + pidx(to, b))

    remote(dact.at[0], dact.at[1], das, dar, tp=other).wait_recv()
    for kb_ in (1, 3, 2, 0):
        g = (b + kb_) % 4
        other_act = jnp.concatenate([dact[1, i * 4 + g] for i in range(4)], axis=0)
        part = dot(dact[0, pl.ds(g * 4, 4)].reshape(128, 256)[:, :192], ddg[c].reshape(192, HALF)) + dot(
            other_act[:, :192], ddg[other].reshape(192, HALF)
        )
        pb[g] = (part * gsc[g][:, 0:1]).astype(BF).reshape(4, ROWS, HALF)
        if kb_:
            r1_copy(kb_).start()

    for cp in later[1:]:
        cp.wait()
    for dy in (0, 1, 3, 2):
        rows = pl.ds(((y + 4 - dy) % 4) * 4, 4)
        remote(X.at[rows], Xo.at[rows], xds.at[dy], xdr.at[dy], tp=other).wait_recv()
    own_rows = X[...].reshape(256, HALF)
    other_rows = Xo[...].reshape(256, HALF)
    gate_pre = dot_nt(own_rows, eg[:, half]) + dot_nt(other_rows, eg[:, other_half])
    up_pre = dot_nt(own_rows, eu[:, half]) + dot_nt(other_rows, eu[:, other_half])
    inner = gate_pre / (1.0 + jnp.exp(-gate_pre)) * up_pre
    abuf[0] = jnp.concatenate([inner, jnp.zeros((256, 32), F32)], axis=1).astype(BF)
    a_copy = remote(abuf.at[0], abuf.at[1], as_, ar, tp=other)
    a_copy.start()
    own_ed = ed[pl.ds(pl.multiple_of(c * 352, 32), 352), :]
    other_ed = ed[pl.ds(pl.multiple_of(other * 352, 32), 352), :]
    down = dot(abuf[0][:, :352], own_ed)
    remote(abuf.at[0], abuf.at[1], as_, ar, tp=other).wait_recv()
    down = down + dot(abuf[1][:, :352], other_ed)
    Y[...] = down.astype(BF).reshape(16, 16, HALF)

    for dy, dx in MATES:
        y_copy(dy, dx).start()
    R[p0] = Y[p0]
    for k in NEAR:
        r1_copy(k).wait_recv()
    tb[...] = (
        pb[b].astype(F32) + s1[0].astype(F32) + s1[1].astype(F32) + s1[2].astype(F32)
    ).astype(BF)
    for k in NEAR:
        r2_copy(k).start()
    for dy, dx in MATES:
        i = dy * 4 + dx
        ref = R.at[mate(-dy, -dx)]
        remote(ref, ref, ys.at[i], yr.at[i], tp=other).wait_recv()
    M[...] = dot_tn(selw[...], R[...].reshape(256, HALF)).astype(BF).reshape(4, ROWS, HALF)

    def m_copy(k):
        return remote(M.at[(z + k) % 4], m_in.at[k - 1], ms.at[k], mr.at[k], ep=z_ep(k))

    for k in NEAR:
        m_copy(k).start()
    for k in NEAR:
        r2_copy(k).wait_recv()
    final = tb[a].astype(F32) + s2[0].astype(F32) + s2[1].astype(F32) + s2[2].astype(F32)
    final = resid[:, half] + final + M[z].astype(F32)
    for k in NEAR:
        m_copy(k).wait_recv()
    final = final + m_in[0].astype(F32) + m_in[1].astype(F32) + m_in[2].astype(F32)
    out[:, :HALF] = final.astype(BF)

    for i in range(8):
        w_copy(i).wait_send()
    for k in NEAR:
        rt_copy(k).wait_send()
        zg_copy(k).wait_send()
        m_copy(k).wait_send()
        g_copy(0, 0, k, 0).wait_send()
        g_copy(0, 0, 0, k).wait_send()
        r1_copy(k).wait_send()
        r2_copy(k).wait_send()
        for i in NEAR:
            g_copy(i, 0, 0, k).wait_send()
    for dy, dx in MATES:
        x_copy(dy, dx).wait_send()
        y_copy(dy, dx).wait_send()
        g_share(dy, dx).wait_send()
    for k in range(4):
        x_share(k).wait_send()
    act_copy.wait_send()
    a_copy.wait_send()


def split_kernel(both, out, nk, nv, sem):
    copies = [
        pltpu.make_async_copy(both.at[:, pl.ds(0, HALF)], out, sem.at[0]),
        pltpu.make_async_copy(both.at[:, pl.ds(HALF, 128)], nk, sem.at[1]),
        pltpu.make_async_copy(both.at[:, pl.ds(HALF + 128, 128)], nv, sem.at[2]),
    ]
    for cp in copies:
        cp.start()
    for cp in copies:
        cp.wait()


def per_device(
    hidden_in, past_lengths, key_cache, value_cache, attn_gain, w_query, w_key, w_value,
    lambdas, head_gain, w_out, ffn_gain, route_ids, route_weights, expert_gate, expert_up,
    expert_down, gate_vector, dense_gate, dense_up, dense_down,
):
    freq = np.power(np.float32(ROPE_BASE), -(np.arange(128) % 32).astype(np.float32) / np.float32(32))
    freq = jnp.asarray(freq.astype(np.float32)[None])
    vm = pl.BlockSpec(memory_space=pltpu.VMEM)
    sm = pl.BlockSpec(memory_space=pltpu.SMEM)
    hbm = pl.BlockSpec(memory_space=pl.ANY)
    V = pltpu.VMEM
    dma = pltpu.SemaphoreType.DMA
    scratch = [
        V((ROWS, CACHE, 128), BF), V((ROWS, CACHE, 128), BF),
        V((WIDTH, 1024), BF), V((WIDTH, 128), BF), V((WIDTH, 128), BF), V((1024, WIDTH), BF),
        V((352, WIDTH), BF), V((352, WIDTH), BF), V((704, HALF), BF),
        V((44, WIDTH), BF), V((44, WIDTH), BF), V((48, HALF), BF),
        V((2, 4, 48, WIDTH), BF), V((2, 4, 48, HALF), BF),
        V((ROWS, 8, 128), F32), V((ROWS, 128), F32), V((ROWS, 128), F32), V((ROWS, 8, 128), F32),
        V((2, ROWS, WIDTH), BF), V((ROWS, WIDTH), F32), V((4, 8, 128), F32),
        V((16, ROWS, WIDTH), BF), V((4, ROWS, HALF), BF), V((16, 16, HALF), BF),
        V((16, 16, HALF), BF), V((16, 16, HALF), BF), V((2, 256, 384), BF), V((16, 16, HALF), BF),
        V((16, 16, HALF), BF), V((4, ROWS, HALF), BF), V((3, ROWS, HALF), BF),
        V((2, 16, ROWS, 256), BF), V((4, 128, 128), F32), V((256, 128), BF), V((256, 128), BF),
        V((4, 4, ROWS, HALF), BF), V((3, 4, ROWS, HALF), BF), V((4, ROWS, HALF), BF),
        V((3, ROWS, HALF), BF),
        dma((11,)), dma((2, NGRP)), dma((8,)), dma((8,)), dma, dma,
        dma((4,)), dma((4,)),
        dma((16,)), dma((16,)), dma((16,)), dma((16,)), dma((4,)), dma((4,)), dma((16,)), dma((16,)),
        dma((4,)), dma((4,)), dma, dma, dma, dma, dma((16,)), dma((16,)),
        dma((4,)), dma((4,)), dma((4,)), dma((4,)), dma((4,)), dma((4,)),
    ]
    both = pl.pallas_call(
        layer_kernel,
        name="layer",
        out_shape=jax.ShapeDtypeStruct((ROWS, HALF + 256), BF),
        in_specs=[vm, vm, sm, vm, vm, sm, vm, vm, vm, vm, vm] + [hbm] * 12,
        out_specs=vm,
        scratch_shapes=scratch,
        compiler_params=pltpu.CompilerParams(
            collective_id=0, has_side_effects=True, vmem_limit_bytes=VMEM_BYTES
        ),
    )(
        hidden_in, freq, past_lengths, past_lengths.reshape(1, ROWS), attn_gain.reshape(1, WIDTH),
        lambdas, head_gain.reshape(1, 128), ffn_gain.reshape(1, WIDTH), route_ids.T,
        route_weights.T, gate_vector.reshape(16, 128),
        key_cache, value_cache, w_query, w_key, w_value, w_out,
        expert_gate.swapaxes(1, 2), expert_up.swapaxes(1, 2), expert_down,
        dense_gate.T, dense_up.T, dense_down,
    )
    return pl.pallas_call(
        split_kernel,
        name="split",
        out_shape=(
            jax.ShapeDtypeStruct((ROWS, HALF), BF),
            jax.ShapeDtypeStruct((ROWS, 128), BF),
            jax.ShapeDtypeStruct((ROWS, 128), BF),
        ),
        in_specs=[hbm],
        out_specs=(hbm, hbm, hbm),
        scratch_shapes=[dma((3,))],
        compiler_params=pltpu.CompilerParams(vmem_limit_bytes=1 << 20),
    )(both)


def solution(mesh):
    return jax.shard_map(
        per_device,
        mesh=mesh,
        in_specs=(
            P("ep", None), P("ep"), P("ep", None, "tp"), P("ep", None, "tp"), P(),
            P(None, "tp"), P(None, "tp"), P(None, "tp"), P("tp"), P(), P("tp", None), P(),
            P("ep", None), P("ep", None), P("ep", None, "tp"), P("ep", None, "tp"),
            P("ep", None, "tp"), P(), P(None, ("ep", "tp")), P(None, ("ep", "tp")), P("ep", "tp"),
        ),
        out_specs=(P("ep", "tp"), P("ep", "tp"), P("ep", "tp")),
        check_vma=False,
    )
```

```python
import jax
import jax.numpy as jnp
import numpy as np
from jax import lax
from jax.experimental import pallas as pl
from jax.experimental.pallas import tpu as pltpu
from jax.sharding import PartitionSpec as P

EPS = 1e-05
ROPE_BASE = 10000.0
BF = jnp.bfloat16
F32 = jnp.float32
ROWS = 32
WIDTH = 2048
HALF = 1024
CACHE = 1024
GRP = 8
NGRP = ROWS // GRP
AHEAD = 4
VMEM_BYTES = 66 * 1000 * 1000
NEAR = (2, 1, 3)
FAR = (2, 1, 3)
MATES = tuple((i // 4, i % 4) for i in (10, 6, 14, 9, 11, 2, 8, 5, 7, 13, 15, 1, 3, 4, 12))
NT = (((1,), (1,)), ((), ()))
TN = (((0,), (0,)), ((), ()))


def dot(a, b):
    return jnp.dot(a, b, preferred_element_type=F32)


def dot_nt(a, b):
    return lax.dot_general(a, b, NT, preferred_element_type=F32)


def dot_tn(a, b):
    return lax.dot_general(a, b, TN, preferred_element_type=F32)


def layer_kernel(
    hid, freq, plen, prow, again, lam, hgain, fgain, ids, wts, gvec,
    kc_h, vc_h, wq_h, wk_h, wv_h, wo_h, eg_h, eu_h, ed_h, dg_h, du_h, dd_h,
    out,
    kb, vb, wq, wk, wv, wo, eg, eu, ed, dg, du, dtail,
    wdg, ddg, qs, kn, vn, ho, pbuf, resid, rt, G, zg, D, X, Xo, abuf, Y, R, M, m_in,
    dact, gsc, sel, selw, pb, s1, tb, s2,
    lsem, wqsem, kvsem, wss, wrs, tps, tpr, rts, rtr,
    gss, grs, gds, gdr, zs, zr, xs, xr, xds, xdr, as_, ar, das, dar, ys, yr,
    r1s, r1r, r2s, r2r, ms, mr,
):
    c = lax.axis_index("tp")
    ep = lax.axis_index("ep")
    z = ep // 16
    p0 = ep % 16
    y = p0 // 4
    x = p0 % 4
    sa = 1 + 3 * c
    sb = 4 - 3 * c
    a = x * (1 - c) + y * c
    b = y * (1 - c) + x * c
    zb = z * 16
    other = 1 - c
    half = pl.ds(pl.multiple_of(c * HALF, HALF), HALF)
    other_half = pl.ds(pl.multiple_of(other * HALF, HALF), HALF)

    def local(src, dst, sem):
        return pltpu.make_async_copy(src, dst, sem)

    def remote(src, dst, ssem, rsem, **dev):
        return pltpu.make_async_remote_copy(
            src_ref=src, dst_ref=dst, send_sem=ssem, recv_sem=rsem,
            device_id=dev, device_id_type=pl.DeviceIdType.MESH,
        )

    def pidx(aa, bb):
        return aa * sa + bb * sb

    def z_ep(step):
        return ((z + 4 + step) % 4) * 16 + p0

    own_w = [
        local(dg_h, dg, lsem.at[3]),
        local(du_h, du, lsem.at[4]),
        local(dd_h.at[pl.ds(0, 48)], ddg.at[0, z], lsem.at[9]),
        local(dd_h.at[pl.ds(40, 48)], dtail, lsem.at[10]),
    ]
    first = [
        local(wk_h, wk, lsem.at[1]),
        local(wv_h, wv, lsem.at[2]),
    ]
    first += [
        local(wq_h.at[:, pl.ds(i * 256, 256)], wq.at[:, pl.ds(i * 256, 256)], wqsem.at[i])
        for i in range(4)
    ]
    for cp in own_w + first:
        cp.start()

    def kv(g):
        rows = pl.ds(g * GRP, GRP)
        return (
            local(kc_h.at[rows], kb.at[rows], kvsem.at[0, g]),
            local(vc_h.at[rows], vb.at[rows], kvsem.at[1, g]),
        )

    later = [
        local(wo_h, wo, lsem.at[5]),
        local(eg_h.at[0], eg, lsem.at[6]),
        local(eu_h.at[0], eu, lsem.at[7]),
        local(ed_h.at[0], ed, lsem.at[8]),
    ]

    barrier = pltpu.get_barrier_semaphore()
    for k in range(1, 16):
        dest = zb + ((y + k // 4) % 4) * 4 + (x + k % 4) % 4
        pl.semaphore_signal(barrier, inc=1, device_id={"ep": dest}, device_id_type=pl.DeviceIdType.MESH)
    for step in NEAR:
        pl.semaphore_signal(barrier, inc=1, device_id={"ep": z_ep(step)}, device_id_type=pl.DeviceIdType.MESH)
    pl.semaphore_signal(barrier, inc=1, device_id={"tp": other}, device_id_type=pl.DeviceIdType.MESH)

    at = lax.broadcasted_iota(jnp.int32, (ROWS, 128), 0)
    lane = lax.broadcasted_iota(jnp.int32, (ROWS, 128), 1)
    diag = at == lane
    shifted = at + 32 * z == lane

    def lanes(v, fill):
        return jnp.concatenate([v.astype(F32), jnp.full((v.shape[0], 128 - ROWS), fill, F32)], axis=1)

    def column(v):
        return jnp.sum(jnp.where(diag, v, 0.0), axis=1, keepdims=True)

    def moved(col):
        return jnp.sum(jnp.where(shifted, col, 0.0), axis=0, keepdims=True)

    id_rows = lanes(ids[...], -1.0)
    wt_rows = lanes(wts[...], 0.0)
    earlier = lane < at
    facts = []
    for k in range(2):
        col = column(id_rows[k : k + 1])
        same = jnp.where(id_rows[0:1] == col, 1.0, 0.0) + jnp.where(id_rows[1:2] == col, 1.0, 0.0)
        rank = jnp.sum(jnp.where(earlier, same, 0.0), axis=1, keepdims=True)
        facts.append(moved(col * 4.0 + rank))
    for k in range(2):
        facts.append(moved(column(wt_rows[k : k + 1])))
    facts.append(jnp.zeros((4, 128), F32))
    rt[z] = jnp.concatenate(facts, axis=0)

    h = hid[...].astype(F32)
    normed = (h * lax.rsqrt(jnp.mean(h * h, axis=-1, keepdims=True) + EPS) * again[...]).astype(BF)
    angles = column(lanes(prow[...], 0.0)) * freq[...]
    cos = jnp.cos(angles)
    low = (lane & 63) < 32
    sin = jnp.sin(angles) * jnp.where(low, -1.0, 1.0)

    for g in range(AHEAD):
        for cp in kv(g):
            cp.start()

    for cp in own_w:
        cp.wait()
    gv = gvec[...].astype(F32)
    gv = jnp.concatenate([gv[i : i + 1] for i in range(16)], axis=1)
    pad_row = lax.broadcasted_iota(jnp.int32, (4, WIDTH), 0)
    wdg[0, z, 0:44, :] = dg[...]
    wdg[0, z, 44:48, :] = jnp.where(pad_row == 0, gv, 0.0).astype(BF)
    wdg[1, z, 0:44, :] = du[...]
    wdg[1, z, 44:48, :] = jnp.zeros((4, WIDTH), BF)
    ddg[1, z] = pltpu.roll(dtail[...].astype(F32), 44, 0).astype(BF)

    pl.semaphore_wait(barrier, 19)

    def rt_copy(k):
        return remote(rt.at[z], rt.at[z], rts.at[k], rtr.at[k], ep=z_ep(k))

    for k in NEAR:
        rt_copy(k).start()

    def w_copy(i):
        block = (z + 4 + (0, 0, 0, 0, -1, 1, -1, 1)[i]) % 4
        ref = (
            wdg.at[:, block], wdg.at[:, block], ddg.at[:, block], ddg.at[:, block],
            wdg.at[0, block], wdg.at[1, block], ddg.at[0, block], ddg.at[1, block],
        )[i]
        return remote(ref, ref, wss.at[i], wrs.at[i], ep=z_ep((1, -1)[i % 2]))

    def w_wait(i):
        block = (z + 4 + (-1, 1, -1, 1, -2, 2, -2, 2)[i]) % 4
        ref = (
            wdg.at[:, block], wdg.at[:, block], ddg.at[:, block], ddg.at[:, block],
            wdg.at[0, block], wdg.at[1, block], ddg.at[0, block], ddg.at[1, block],
        )[i]
        remote(ref, ref, wss.at[i], wrs.at[i], tp=other).wait_recv()

    for i in (2, 3, 0, 1):
        w_copy(i).start()

    def rotated(v):
        turned = jnp.where(low, pltpu.roll(v, 96, 1), pltpu.roll(v, 32, 1))
        return (v * cos + turned * sin).astype(BF)

    for cp in first[:2]:
        cp.wait()
    new_k = rotated(dot(normed, wk[...]))
    new_v = dot(normed, wv[...]).astype(BF)
    out[:, HALF : HALF + 128] = new_k
    out[:, HALF + 128 : HALF + 256] = new_v
    kn[...] = new_k.astype(F32)
    vn[...] = new_v.astype(F32)
    for i in range(4):
        first[2 + i].wait()
        q = dot(normed, wq[:, i * 256 : i * 256 + 256])
        for j in range(2):
            qs[:, 2 * i + j, :] = rotated(q[:, j * 128 : j * 128 + 128]).astype(F32) * 0.125

    lam_col = jnp.zeros((8, 128), F32)
    rows8 = lax.broadcasted_iota(jnp.int32, (8, 128), 0)
    for i in range(8):
        lam_col = jnp.where(rows8 == i, lam[i], lam_col)
    left = lax.broadcasted_iota(jnp.int32, (8, 128), 1) < 64
    last16 = lax.broadcasted_iota(jnp.int32, (16, 128), 0) == 15
    places = lax.broadcasted_iota(jnp.int32, (16, CACHE), 1)
    gain = hgain[...]

    @pl.loop(0, NGRP)
    def _(g):
        for cp in kv(g):
            cp.wait()

        @pl.when(g + AHEAD < NGRP)
        def _():
            for cp in kv(g + AHEAD):
                cp.start()

        @pl.when(g + AHEAD == NGRP)
        def _():
            later[0].start()

        sums, parts = [], []
        for i in range(GRP):
            s = g * GRP + i
            tail = pl.ds(CACHE - 16, 16)
            kb[s, tail, :] = jnp.where(
                last16, jnp.broadcast_to(kn[pl.ds(s, 1), :], (16, 128)), kb[s, tail, :].astype(F32)
            ).astype(BF)
            vb[s, tail, :] = jnp.where(
                last16, jnp.broadcast_to(vn[pl.ds(s, 1), :], (16, 128)), vb[s, tail, :].astype(F32)
            ).astype(BF)
            qv = qs[s]
            q2 = jnp.concatenate(
                [jnp.where(left, qv, 0.0), jnp.where(left, 0.0, qv)], axis=0
            ).astype(BF)
            scores = dot_nt(q2, kb[s])
            usable = (places < plen[s]) | (places == CACHE - 1)
            scores = jnp.where(usable, scores, -jnp.inf)
            peak = jnp.max(scores, axis=-1, keepdims=True)
            weights = jnp.exp(scores - peak)
            sums.append(jnp.sum(weights, axis=-1, keepdims=True))
            parts.append(weights.astype(BF))
        for i in range(0, GRP, 2):
            s = g * GRP + i
            values = jnp.concatenate([vb[s], vb[s + 1]], axis=1)
            pair = dot(jnp.concatenate(parts[i : i + 2], axis=0), values)
            for j in range(2):
                mapped = pair[16 * j : 16 * j + 16, 128 * j : 128 * j + 128] / sums[i + j]
                mix = mapped[0:8] - lam_col * mapped[8:16]
                ho[s + j] = mix * lax.rsqrt(jnp.mean(mix * mix, axis=-1, keepdims=True) + EPS) * gain

    for cp in later[1:]:
        cp.start()
    later[0].wait()
    head_out = jnp.concatenate([ho[:, i, :].astype(BF) for i in range(8)], axis=1)
    pbuf[0] = dot(head_out, wo[...]).astype(BF)
    tp_copy = remote(pbuf.at[0], pbuf.at[1], tps, tpr, tp=other)
    tp_copy.start()
    tp_copy.wait()
    attn_out = (pbuf[0].astype(F32) + pbuf[1].astype(F32)).astype(BF)
    res = hid[...].astype(F32) + attn_out.astype(F32)
    resid[...] = res
    G[b * 4 + a] = (
        res * lax.rsqrt(jnp.mean(res * res, axis=-1, keepdims=True) + EPS) * fgain[...]
    ).astype(BF)

    def g_copy(ka, kb_, da, db):
        src = ((b + 4 - kb_) % 4) * 4 + (a + 4 - ka) % 4
        dest = zb + pidx((a + da) % 4, (b + db) % 4)
        i = (ka + da) * 4 + kb_ + db
        ref = G.at[src, :, half]
        return remote(ref, ref, gss.at[i], grs.at[i], ep=dest)

    def g_share(ka, kb_):
        aa, bb = (a + 4 - ka) % 4, (b + 4 - kb_) % 4
        i = kb_ * 4 + ka
        return remote(
            G.at[bb * 4 + aa, :, half], G.at[aa * 4 + bb, :, half], gds.at[i], gdr.at[i], tp=other
        )

    def g_arrive(ka, kb_):
        i = ka * 4 + kb_
        ref = G.at[((b + 4 - kb_) % 4) * 4 + (a + 4 - ka) % 4, :, half]
        remote(ref, ref, gss.at[i], grs.at[i], tp=other).wait_recv()
        g_share(ka, kb_).start()

    own_block = G.at[b * 4 + a, :, half]

    def zg_copy(k):
        return remote(own_block, zg.at[z], zs.at[k], zr.at[k], ep=z_ep(k))

    for k in FAR:
        g_copy(0, 0, k, 0).start()
        zg_copy(k).start()
    zg[z] = G[b * 4 + a, :, half]

    for k in NEAR:
        ref = rt.at[(z + 4 - k) % 4]
        remote(ref, ref, rts.at[k], rtr.at[k], tp=other).wait_recv()
    facts = rt[0] + rt[1] + rt[2] + rt[3]
    row = lax.broadcasted_iota(jnp.int32, (256, 128), 0)
    token = lax.broadcasted_iota(jnp.int32, (256, 128), 1)
    target = (((zb + (row >> 4)) >> 1) * 4 + (row & 3)).astype(F32)
    mine = ((row >> 2) & 3) == (token >> 5)
    hit0 = mine & (facts[0:1] == target)
    hit1 = mine & (facts[1:2] == target)
    sel[...] = jnp.where(hit0 | hit1, 1.0, 0.0).astype(BF)
    selw[...] = (jnp.where(hit0, facts[2:3], 0.0) + jnp.where(hit1, facts[3:4], 0.0)).astype(BF)

    for i in (2, 3):
        w_wait(i)
        w_copy(4 + i).start()

    for ka in NEAR:
        g_arrive(ka, 0)
        if ka == NEAR[0]:
            for k in NEAR:
                g_copy(0, 0, 0, k).start()
    for k in NEAR:
        for ka in NEAR:
            g_copy(ka, 0, 0, k).start()

    def mate(dy, dx):
        return ((y + 4 + dy) % 4) * 4 + (x + 4 + dx) % 4

    def x_copy(dy, dx):
        i = dy * 4 + dx
        to = mate(dy, dx)
        return remote(D.at[to], X.at[p0], xs.at[i], xr.at[i], ep=zb + to)

    def y_copy(dy, dx, n):
        i = dy * 4 + dx
        to = mate(dy, dx)
        cols = pl.ds(n * 512, 512)
        return remote(Y.at[to, :, cols], R.at[p0, :, cols], ys.at[n, i], yr.at[n, i], ep=zb + to)

    for k in NEAR:
        ref = zg.at[(z + 4 - k) % 4]
        remote(ref, ref, zs.at[k], zr.at[k], tp=other).wait_recv()
    D[...] = dot(sel[...], zg[...].reshape(128, HALF)).astype(BF).reshape(16, 16, HALF)
    for dy, dx in MATES:
        x_copy(dy, dx).start()
    for i in (0, 1):
        w_wait(i)
        w_copy(4 + i).start()
    X[p0] = D[p0]

    for k in NEAR:
        for ka in (0, 2, 1, 3):
            g_arrive(ka, k)
    for i in range(4, 8):
        w_wait(i)
    for ka in range(4):
        for kb_ in range(4):
            if ka or kb_:
                i = ka * 4 + kb_
                ref = G.at[((b + 4 - kb_) % 4) * 4 + (a + 4 - ka) % 4, :, other_half]
                remote(ref, ref, gds.at[i], gdr.at[i], tp=other).wait_recv()

    @pl.loop(0, 4)
    def _(g):
        tokens = G[pl.ds(g * 4, 4)].reshape(128, WIDTH)
        pre_gate = dot_nt(tokens, wdg[0].reshape(192, WIDTH))
        pre_up = dot_nt(tokens, wdg[1].reshape(192, WIDTH))
        act = pre_gate / (1.0 + jnp.exp(-pre_gate)) * pre_up
        act = jnp.concatenate([act, jnp.zeros((128, 64), F32)], axis=1).astype(BF)
        dact[0, pl.ds(g * 4, 4)] = act.reshape(4, ROWS, 256)
        mix_gate = (1.0 / (1.0 + jnp.exp(-pre_gate[:, 44:45]))).astype(BF).astype(F32)
        gsc[g] = jnp.broadcast_to(mix_gate, (128, 128))

    act_copy = remote(dact.at[0], dact.at[1], das, dar, tp=other)
    act_copy.start()

    def r1_copy(k):
        to = (b + k) % 4
        return remote(pb.at[to], s1.at[k - 1], r1s.at[k], r1r.at[k], ep=zb + pidx(a, to))

    def r2_copy(k):
        to = (a + k) % 4
        return remote(tb.at[to], s2.at[k - 1], r2s.at[k], r2r.at[k], ep=zb + pidx(to, b))

    remote(dact.at[0], dact.at[1], das, dar, tp=other).wait_recv()
    for kb_ in (2, 1, 3, 0):
        g = (b + kb_) % 4
        other_act = jnp.concatenate([dact[1, i * 4 + g] for i in range(4)], axis=0)
        part = dot(dact[0, pl.ds(g * 4, 4)].reshape(128, 256)[:, :192], ddg[c].reshape(192, HALF)) + dot(
            other_act[:, :192], ddg[other].reshape(192, HALF)
        )
        pb[g] = (part * gsc[g][:, 0:1]).astype(BF).reshape(4, ROWS, HALF)
        if kb_:
            r1_copy(kb_).start()

    def x_share(dy):
        rows = pl.ds(((y + 4 - dy) % 4) * 4, 4)
        return remote(X.at[rows], Xo.at[rows], xds.at[dy], xdr.at[dy], tp=other)

    for dy in (0, 1, 3, 2):
        for dx in range(4):
            if dy or dx:
                i = dy * 4 + dx
                ref = X.at[mate(-dy, -dx)]
                remote(ref, ref, xs.at[i], xr.at[i], tp=other).wait_recv()
        x_share(dy).start()

    for cp in later[1:]:
        cp.wait()
    own_rows = X[...].reshape(256, HALF)
    gate_pre = dot_nt(own_rows, eg[:, half])
    up_pre = dot_nt(own_rows, eu[:, half])
    for dy in (0, 1, 3, 2):
        rows = pl.ds(((y + 4 - dy) % 4) * 4, 4)
        remote(X.at[rows], Xo.at[rows], xds.at[dy], xdr.at[dy], tp=other).wait_recv()
    other_rows = Xo[...].reshape(256, HALF)
    gate_pre = gate_pre + dot_nt(other_rows, eg[:, other_half])
    up_pre = up_pre + dot_nt(other_rows, eu[:, other_half])
    inner = gate_pre / (1.0 + jnp.exp(-gate_pre)) * up_pre
    abuf[0] = jnp.concatenate([inner, jnp.zeros((256, 32), F32)], axis=1).astype(BF)
    a_copy = remote(abuf.at[0], abuf.at[1], as_, ar, tp=other)
    a_copy.start()
    own_ed = ed[pl.ds(pl.multiple_of(c * 352, 32), 352), :]
    other_ed = ed[pl.ds(pl.multiple_of(other * 352, 32), 352), :]
    down = [dot(abuf[0][:, :352], own_ed[:, n * 512 : n * 512 + 512]) for n in range(2)]
    remote(abuf.at[0], abuf.at[1], as_, ar, tp=other).wait_recv()

    for n in range(2):
        cols = slice(n * 512, n * 512 + 512)
        part = down[n] + dot(abuf[1][:, :352], other_ed[:, cols])
        Y[:, :, cols] = part.astype(BF).reshape(16, 16, 512)
        for dy, dx in MATES:
            y_copy(dy, dx, n).start()
    R[p0] = Y[p0]
    for k in NEAR:
        r1_copy(k).wait_recv()
    tb[...] = (
        pb[b].astype(F32) + s1[0].astype(F32) + s1[1].astype(F32) + s1[2].astype(F32)
    ).astype(BF)
    for k in FAR:
        r2_copy(k).start()
    def m_copy(k, n):
        cols = pl.ds(n * 512, 512)
        return remote(
            M.at[(z + k) % 4, :, cols], m_in.at[k - 1, :, cols], ms.at[n, k], mr.at[n, k], ep=z_ep(k)
        )

    for n in range(2):
        for dy, dx in MATES:
            i = dy * 4 + dx
            ref = R.at[mate(-dy, -dx), :, pl.ds(n * 512, 512)]
            remote(ref, ref, ys.at[n, i], yr.at[n, i], tp=other).wait_recv()
        cols = slice(n * 512, n * 512 + 512)
        M[:, :, cols] = dot_tn(selw[...], R[:, :, cols].reshape(256, 512)).astype(BF).reshape(4, ROWS, 512)
        for k in FAR:
            m_copy(k, n).start()
    for k in NEAR:
        r2_copy(k).wait_recv()
    final = tb[a].astype(F32) + s2[0].astype(F32) + s2[1].astype(F32) + s2[2].astype(F32)
    final = resid[:, half] + final + M[z].astype(F32)
    for k in NEAR:
        for n in range(2):
            m_copy(k, n).wait_recv()
    final = final + m_in[0].astype(F32) + m_in[1].astype(F32) + m_in[2].astype(F32)
    out[:, :HALF] = final.astype(BF)

    for i in range(8):
        w_copy(i).wait_send()
    for k in NEAR:
        rt_copy(k).wait_send()
        zg_copy(k).wait_send()
        for n in range(2):
            m_copy(k, n).wait_send()
        g_copy(0, 0, k, 0).wait_send()
        g_copy(0, 0, 0, k).wait_send()
        r1_copy(k).wait_send()
        r2_copy(k).wait_send()
        for i in NEAR:
            g_copy(i, 0, 0, k).wait_send()
    for dy, dx in MATES:
        x_copy(dy, dx).wait_send()
        for n in range(2):
            y_copy(dy, dx, n).wait_send()
        g_share(dy, dx).wait_send()
    for k in range(4):
        x_share(k).wait_send()
    act_copy.wait_send()
    a_copy.wait_send()


def split_kernel(both, out, nk, nv, sem):
    copies = [
        pltpu.make_async_copy(both.at[:, pl.ds(0, HALF)], out, sem.at[0]),
        pltpu.make_async_copy(both.at[:, pl.ds(HALF, 128)], nk, sem.at[1]),
        pltpu.make_async_copy(both.at[:, pl.ds(HALF + 128, 128)], nv, sem.at[2]),
    ]
    for cp in copies:
        cp.start()
    for cp in copies:
        cp.wait()


def per_device(
    hidden_in, past_lengths, key_cache, value_cache, attn_gain, w_query, w_key, w_value,
    lambdas, head_gain, w_out, ffn_gain, route_ids, route_weights, expert_gate, expert_up,
    expert_down, gate_vector, dense_gate, dense_up, dense_down,
):
    freq = np.power(np.float32(ROPE_BASE), -(np.arange(128) % 32).astype(np.float32) / np.float32(32))
    freq = jnp.asarray(freq.astype(np.float32)[None])
    vm = pl.BlockSpec(memory_space=pltpu.VMEM)
    sm = pl.BlockSpec(memory_space=pltpu.SMEM)
    hbm = pl.BlockSpec(memory_space=pl.ANY)
    V = pltpu.VMEM
    dma = pltpu.SemaphoreType.DMA
    scratch = [
        V((ROWS, CACHE, 128), BF), V((ROWS, CACHE, 128), BF),
        V((WIDTH, 1024), BF), V((WIDTH, 128), BF), V((WIDTH, 128), BF), V((1024, WIDTH), BF),
        V((352, WIDTH), BF), V((352, WIDTH), BF), V((704, HALF), BF),
        V((44, WIDTH), BF), V((44, WIDTH), BF), V((48, HALF), BF),
        V((2, 4, 48, WIDTH), BF), V((2, 4, 48, HALF), BF),
        V((ROWS, 8, 128), F32), V((ROWS, 128), F32), V((ROWS, 128), F32), V((ROWS, 8, 128), F32),
        V((2, ROWS, WIDTH), BF), V((ROWS, WIDTH), F32), V((4, 8, 128), F32),
        V((16, ROWS, WIDTH), BF), V((4, ROWS, HALF), BF), V((16, 16, HALF), BF),
        V((16, 16, HALF), BF), V((16, 16, HALF), BF), V((2, 256, 384), BF), V((16, 16, HALF), BF),
        V((16, 16, HALF), BF), V((4, ROWS, HALF), BF), V((3, ROWS, HALF), BF),
        V((2, 16, ROWS, 256), BF), V((4, 128, 128), F32), V((256, 128), BF), V((256, 128), BF),
        V((4, 4, ROWS, HALF), BF), V((3, 4, ROWS, HALF), BF), V((4, ROWS, HALF), BF),
        V((3, ROWS, HALF), BF),
        dma((11,)), dma((4,)), dma((2, NGRP)), dma((8,)), dma((8,)), dma, dma,
        dma((4,)), dma((4,)),
        dma((16,)), dma((16,)), dma((16,)), dma((16,)), dma((4,)), dma((4,)), dma((16,)), dma((16,)),
        dma((4,)), dma((4,)), dma, dma, dma, dma, dma((2, 16)), dma((2, 16)),
        dma((4,)), dma((4,)), dma((4,)), dma((4,)), dma((2, 4)), dma((2, 4)),
    ]
    both = pl.pallas_call(
        layer_kernel,
        name="layer",
        out_shape=jax.ShapeDtypeStruct((ROWS, HALF + 256), BF),
        in_specs=[vm, vm, sm, vm, vm, sm, vm, vm, vm, vm, vm] + [hbm] * 12,
        out_specs=vm,
        scratch_shapes=scratch,
        compiler_params=pltpu.CompilerParams(
            collective_id=0, has_side_effects=True, vmem_limit_bytes=VMEM_BYTES
        ),
    )(
        hidden_in, freq, past_lengths, past_lengths.reshape(1, ROWS), attn_gain.reshape(1, WIDTH),
        lambdas, head_gain.reshape(1, 128), ffn_gain.reshape(1, WIDTH), route_ids.T,
        route_weights.T, gate_vector.reshape(16, 128),
        key_cache, value_cache, w_query, w_key, w_value, w_out,
        expert_gate.swapaxes(1, 2), expert_up.swapaxes(1, 2), expert_down,
        dense_gate.T, dense_up.T, dense_down,
    )
    return pl.pallas_call(
        split_kernel,
        name="split",
        out_shape=(
            jax.ShapeDtypeStruct((ROWS, HALF), BF),
            jax.ShapeDtypeStruct((ROWS, 128), BF),
            jax.ShapeDtypeStruct((ROWS, 128), BF),
        ),
        in_specs=[hbm],
        out_specs=(hbm, hbm, hbm),
        scratch_shapes=[dma((3,))],
        compiler_params=pltpu.CompilerParams(vmem_limit_bytes=1 << 20),
    )(both)


def solution(mesh):
    return jax.shard_map(
        per_device,
        mesh=mesh,
        in_specs=(
            P("ep", None), P("ep"), P("ep", None, "tp"), P("ep", None, "tp"), P(),
            P(None, "tp"), P(None, "tp"), P(None, "tp"), P("tp"), P(), P("tp", None), P(),
            P("ep", None), P("ep", None), P("ep", None, "tp"), P("ep", None, "tp"),
            P("ep", None, "tp"), P(), P(None, ("ep", "tp")), P(None, ("ep", "tp")), P("ep", "tp"),
        ),
        out_specs=(P("ep", "tp"), P("ep", "tp"), P("ep", "tp")),
        check_vma=False,
    )
```
